256 devices in a mesh: sp: 32 (over z, y), fs: 4 (over x), tp: 2 (over core).
Axes of the slice: x: 4, y: 4, z: 8, core: 2. Of those that a mesh axis runs over, the one named last changes fastest.
Arguments:
- tokens: bfloat16 [16384, 2048], P(('fs', 'sp'), 'tp'), parts along dimension 0, may hold values from -6 to 6
- norm_gain: float32 [2048], replicated, may hold values from 0.1 to 1.9
- w_recur_in: bfloat16 [2048, 1024], P(None, 'tp'), may hold values from -0.125 to 0.125
- conv_weight: float32 [4, 1024], P(None, 'tp'), may hold values from -3 to 3
- w_gate_decay: bfloat16 [16, 64, 64], P('tp'), may hold values from -0.75 to 0.75
- w_gate_input: bfloat16 [16, 64, 64], P('tp'), may hold values from -0.75 to 0.75
- decay_base: float32 [1024], P('tp'), may hold values from 0 to 0.01, as said below
- extra_decay: float32 [16384, 16], P(('fs', 'sp'), 'tp'), parts along dimension 0, may hold values from 0 to 1, as said below
- w_query: bfloat16 [2048, 1024], P(None, 'tp'), may hold values from -1 to 1
- w_key: bfloat16 [2048, 256], P(None, 'tp'), may hold values from -20 to 20
- w_value: bfloat16 [2048, 256], P(None, 'tp'), may hold values from -0.125 to 0.125
- mix_lambda: float32 [8], P('tp'), may hold values from 0.3 to 0.8
- head_gain: float32 [128], replicated, may hold values from 0.1 to 1.9
- w_out_recur: bfloat16 [1024, 2048], P('tp'), may hold values from -0.125 to 0.125
- w_out_attend: bfloat16 [1024, 2048], P('tp'), may hold values from -0.125 to 0.125
- out_gain: float32 [2048], replicated, may hold values from 0.1 to 1.9
Outputs:
- mixed: bfloat16 [16384, 2048], P(('fs', 'sp', 'tp')), parts along dimension 0
The draws below stay inside these ranges and needn't reach their ends.
There are 4 independent parts, one for each index of `fs`. The reference program is written for one: setup_inputs(seed, part) draws one part's arguments, and reference() takes and returns one part's arrays. A program takes and returns all parts, laid end to end along the dimension named above; an argument that names none is the same for every part. Nothing has to cross between parts.
Inputs may be any that keep to these rules, and one draw needn't show every extreme that they name: `decay_base`: positive rates of each channel. `extra_decay`: non-negative added log-decays.
All inputs are finite; a program needn't handle non-finite values.
Results may differ from the reference program's by a relative error of at most 0.012.
The reference program's roundings to bfloat16 on the way (of `scaled`, `conv_in`, `recur_out` and `attend_out`) count: a program that leaves them out, or rounds other values in their place, can miss the bound.
Values may be sent and summed in bfloat16 or wider, within the bound.
No kernel may reach another device: no remote copies, remote signals or barrier semaphores. Data moves between devices by JAX's collectives and lax.ppermute only.
A program may use at most 128 MiB of HBM per device.

```python
import math
import jax
import jax.numpy as jnp
from jax import lax

D = 2048
HEAD = 64
RECURRENT_HEADS = 16
CONV = 4
DA_HEADS = 8
KV_HEADS = 2
TOK_DEV = 128
RG_W = 1024
DV = 128
SEQUENCE_TOKENS = 4096


def draw_decay_base(key, part):
    slow_key, fast_key, pick_key = jax.random.split(jax.random.fold_in(key, 11), 3)
    slow_rate = jax.random.uniform(slow_key, (RG_W,), jnp.float32, 0.05, 0.15) / SEQUENCE_TOKENS
    fast_rate = jnp.exp(jax.random.uniform(fast_key, (RG_W,), jnp.float32, math.log(0.0025), math.log(0.0083)))
    fast_share = 0.5
    chosen = jax.random.uniform(pick_key, (RG_W,), jnp.float32) < fast_share
    return jnp.where(chosen, fast_rate, slow_rate).astype(jnp.float32)


def draw_extra_decay(key, part):
    level_key, rough_key, position_random_key, amount_random_key = jax.random.split(jax.random.fold_in(key, 23), 4)
    block_count = SEQUENCE_TOKENS // TOK_DEV
    levels = jnp.exp(jax.random.uniform(level_key, (block_count,), jnp.float32, math.log(0.15), math.log(0.6))) / SEQUENCE_TOKENS
    per_position = jnp.repeat(levels, TOK_DEV)
    rough = jax.random.uniform(rough_key, (SEQUENCE_TOKENS, RECURRENT_HEADS), jnp.float32, 0.5, 1.5)
    baseline_term = per_position[:, None] * rough
    spike_positions = jax.random.randint(position_random_key, (3,), 0, SEQUENCE_TOKENS)
    spike_magnitudes = jax.random.uniform(amount_random_key, (3, RECURRENT_HEADS), jnp.float32, 0.22, 0.51)
    spike_marks = (jnp.arange(SEQUENCE_TOKENS)[:, None] == spike_positions[None, :]).astype(jnp.float32)
    spike_values = jnp.dot(spike_marks, spike_magnitudes)
    return (baseline_term + spike_values).astype(jnp.float32)


def query_key_pair(key):
    query_seed, key_seed = jax.random.split(jax.random.fold_in(key, 37))
    spread = 1.3 / math.sqrt(D)
    query_weight = jnp.clip(jax.random.normal(query_seed, (D, DA_HEADS * 2 * HEAD), jnp.float32), -6.0, 6.0) * spread
    key_weight = jnp.clip(jax.random.normal(key_seed, (D, KV_HEADS * 2 * HEAD), jnp.float32), -6.0, 6.0) * spread
    return (query_weight, key_weight)


def draw_w_query(key, part):
    return query_key_pair(key)[0].astype(jnp.bfloat16)


def draw_w_key(key, part):
    return query_key_pair(key)[1].astype(jnp.bfloat16)


def block_scale(own_key, dims, shards, low, largest):
    def one(position, shards_of):
        draws = jax.random.uniform(jax.random.fold_in(jax.random.fold_in(own_key, 6), position), (shards_of,), jnp.float32, low / len(shards), largest / len(shards))
        return jnp.repeat(jnp.exp(draws), dims[position] // shards_of).reshape((-1,) + (1,) * (len(dims) - position - 1))

    factor_of = one(*shards[0])
    for cut in shards[1:]:
        factor_of = factor_of * one(*cut)
    return factor_of


def centred(own_key, dims, deviation, reach, shards=(), kind=jnp.bfloat16):
    gain = block_scale(own_key, dims, shards, -0.22, 0.18) if shards else 1.0
    values = jax.random.normal(own_key, dims, jnp.float32) * deviation * gain
    return jnp.minimum(jnp.maximum(values, -reach), reach).astype(kind)


def setup_inputs(seed: int = 0, part: int = 0) -> dict:
    key_of = jax.random.split(jax.random.key(seed), 17)
    own_keys = jax.random.split(jax.random.fold_in(key_of[16], part), 17)
    return {
        "tokens": centred(own_keys[0], (SEQUENCE_TOKENS, D), 1.0, 6.0, ((0, 32), (1, 2))),
        "norm_gain": jnp.clip(1.0 + 0.18 * jax.random.normal(key_of[1], (D,), jnp.float32), 0.1, 1.9),
        "w_recur_in": centred(key_of[2], (D, RG_W), D ** -0.5, 0.125, ((1, 2),)),
        "conv_weight": centred(key_of[3], (CONV, RG_W), CONV ** -0.5, 3.0, ((1, 2),), jnp.float32),
        "w_gate_decay": centred(key_of[4], (RECURRENT_HEADS, HEAD, HEAD), HEAD ** -0.5, 0.75, ((0, 2),)),
        "w_gate_input": centred(key_of[5], (RECURRENT_HEADS, HEAD, HEAD), HEAD ** -0.5, 0.75, ((0, 2),)),
        "decay_base": draw_decay_base(jax.random.fold_in(key_of[16], 71), part),
        "extra_decay": draw_extra_decay(jax.random.fold_in(jax.random.fold_in(key_of[16], part), 71), part),
        "w_query": draw_w_query(jax.random.fold_in(key_of[16], 71), part),
        "w_key": draw_w_key(jax.random.fold_in(key_of[16], 71), part),
        "w_value": centred(key_of[10], (D, KV_HEADS * DV), D ** -0.5, 0.125, ((1, 2),)),
        "mix_lambda": jnp.clip(0.3 + 0.5 * jax.random.uniform(key_of[11], (DA_HEADS,), jnp.float32) ** block_scale(key_of[11], (DA_HEADS,), ((0, 2),), -0.2, 0.2), 0.3, 0.8),
        "head_gain": jnp.clip(1.0 + 0.18 * jax.random.normal(key_of[12], (DV,), jnp.float32), 0.1, 1.9),
        "w_out_recur": centred(key_of[13], (RG_W, D), (RG_W + DA_HEADS * DV) ** -0.5, 0.125, ((0, 2),)),
        "w_out_attend": centred(key_of[14], (DA_HEADS * DV, D), (RG_W + DA_HEADS * DV) ** -0.5, 0.125, ((0, 2),)),
        "out_gain": jnp.clip(1.0 + 0.18 * jax.random.normal(key_of[15], (D,), jnp.float32), 0.1, 1.9),
    }


lru_rate = 8.0
norm_eps = 1e-06

def chain(earlier, later):
    return (earlier[0] * later[0], later[0] * earlier[1] + later[1])

def reference(tokens, norm_gain, w_recur_in, conv_weight, w_gate_decay, w_gate_input, decay_base, extra_decay, w_query, w_key, w_value, mix_lambda, head_gain, w_out_recur, w_out_attend, out_gain):
    flat = tokens.astype(jnp.float32)
    inverse = lax.rsqrt(lax.optimization_barrier(jnp.mean(flat * flat, axis=1, keepdims=True)) + norm_eps)
    scaled = (flat * norm_gain).astype(jnp.bfloat16)

    def project(weight):
        return (jnp.dot(scaled, weight, preferred_element_type=jnp.float32) * inverse).astype(jnp.bfloat16)
    recur_in = project(w_recur_in)
    queries = project(w_query)
    keys = project(w_key)
    values = project(w_value)
    padded = jnp.concatenate([jnp.zeros((CONV - 1, RG_W), jnp.bfloat16), recur_in], axis=0).astype(jnp.float32)
    conv_acc = jnp.zeros((SEQUENCE_TOKENS, RG_W), jnp.float32)
    for offset in range(CONV):
        conv_acc = conv_acc + conv_weight[offset] * padded[offset:offset + SEQUENCE_TOKENS]
    conv_in = conv_acc.astype(jnp.bfloat16)
    blocks = conv_in.astype(jnp.float32).reshape(SEQUENCE_TOKENS, RECURRENT_HEADS, HEAD)
    decay_gate = jax.nn.sigmoid(jnp.einsum('thi,hij->thj', blocks, w_gate_decay.astype(jnp.float32))).reshape(SEQUENCE_TOKENS, RG_W)
    input_gate = jax.nn.sigmoid(jnp.einsum('thi,hij->thj', blocks, w_gate_input.astype(jnp.float32))).reshape(SEQUENCE_TOKENS, RG_W)
    log_decay = -lru_rate * decay_gate * decay_base - jnp.repeat(extra_decay, HEAD, axis=1)
    decay = jnp.exp(log_decay)
    inject = jnp.sqrt(-jnp.expm1(2.0 * log_decay)) * input_gate * conv_in.astype(jnp.float32)
    unused_total, states = lax.associative_scan(chain, (decay, inject), axis=0)
    recur_out = states.astype(jnp.bfloat16)
    group_size = DA_HEADS // KV_HEADS
    query_four = queries.reshape(SEQUENCE_TOKENS, KV_HEADS, group_size, 2, HEAD)
    key_three = keys.reshape(SEQUENCE_TOKENS, KV_HEADS, 2, HEAD).astype(jnp.float32)
    value_three = values.reshape(SEQUENCE_TOKENS, KV_HEADS, DV).astype(jnp.float32)
    block_rows = math.gcd(SEQUENCE_TOKENS, 512)
    positions = jnp.arange(SEQUENCE_TOKENS, dtype=jnp.int32)
    lambdas = mix_lambda.reshape(KV_HEADS, group_size)

    def one_block(index):
        begin = (index * block_rows).astype(jnp.int32)
        query_part = lax.dynamic_slice_in_dim(query_four, begin, block_rows, 0).astype(jnp.float32)
        allowed = (begin + jnp.arange(block_rows, dtype=jnp.int32))[:, None] >= positions[None, :]
        results = []
        for mapping in range(2):
            scores = jnp.einsum('bkgd,tkd->kgbt', query_part[:, :, :, mapping, :], key_three[:, :, mapping, :]) * HEAD ** (-0.5)
            scores = jnp.where(allowed, scores, -jnp.inf)
            peak = lax.optimization_barrier(jnp.max(scores, axis=-1, keepdims=True))
            expo = jnp.exp(scores - peak)
            total = lax.optimization_barrier(jnp.sum(expo, axis=-1))
            rounded = lax.optimization_barrier(expo.astype(jnp.bfloat16)).astype(jnp.float32)
            attend = jnp.einsum('kgbt,tke->bkge', rounded, value_three)
            results.append(attend / jnp.transpose(total, (2, 0, 1))[..., None])
        return results[0] - lambdas[None, :, :, None] * results[1]
    head_out = lax.map(one_block, jnp.arange(SEQUENCE_TOKENS // block_rows, dtype=jnp.int32))
    head_out = head_out.reshape(SEQUENCE_TOKENS, DA_HEADS, DV)
    normed = head_out * lax.rsqrt(lax.optimization_barrier(jnp.mean(head_out * head_out, axis=-1, keepdims=True)) + norm_eps) * head_gain
    attend_out = normed.astype(jnp.bfloat16).reshape(SEQUENCE_TOKENS, DA_HEADS * DV)
    merged = jnp.dot(recur_out, w_out_recur, preferred_element_type=jnp.float32) + jnp.dot(attend_out, w_out_attend, preferred_element_type=jnp.float32)
    final = merged * lax.rsqrt(lax.optimization_barrier(jnp.mean(merged * merged, axis=1, keepdims=True)) + norm_eps) * out_gain
    return final.astype(jnp.bfloat16)
```

```python
import functools

import jax
import jax.numpy as jnp
from jax import lax
from jax.experimental import pallas as pl
from jax.experimental.pallas import tpu as pltpu
from jax.sharding import PartitionSpec as P

D = 2048
HEAD = 64
DV = 128
NY = 4
NZ = 8
lru_rate = 8.0
norm_eps = 1e-06
f32 = jnp.float32
bf16 = jnp.bfloat16


def sp_pairs(dz, dy):
    return [
        (z * NY + y, (z + dz) % NZ * NY + (y + dy) % NY) for z in range(NZ) for y in range(NY)
    ]


def xor_pairs(bit):
    return [(i, i ^ bit) for i in range(NZ * NY)]


def after(value, other):
    return lax.optimization_barrier((value, other))[0]


def attend_block(kv, q_ref, acc_ref, stat_ref, mask, cols):
    keys = kv[:, : 2 * HEAD]
    values_t = kv[:, 2 * HEAD :].T
    for at in range(0, q_ref.shape[0], cols):
        part = pl.ds(at, cols)
        scores = lax.dot_general(
            keys, q_ref[part, :], (((1,), (1,)), ((), ())), preferred_element_type=f32
        )
        if mask is not None:
            scores = jnp.where(mask, scores, -1e30)
        old = stat_ref[0:1, part]
        peak = jnp.maximum(old, jnp.max(scores, axis=0, keepdims=True))
        fix = jnp.exp(old - peak)
        expo = jnp.exp(scores - peak)
        stat_ref[0:1, part] = peak
        stat_ref[1:2, part] = stat_ref[1:2, part] * fix + jnp.sum(expo, axis=0, keepdims=True)
        gained = jnp.dot(values_t, expo.astype(bf16), preferred_element_type=f32)
        acc_ref[:, part] = acc_ref[:, part] * fix + gained


def first_kernel(index_ref, q_ref, kv_ref, wide_ref, acc_ref, stat_ref):
    rows = q_ref.shape[0]
    lane = lax.broadcasted_iota(jnp.int32, (rows, 2 * HEAD), 1)
    heads = q_ref.shape[1] // (2 * HEAD)
    for mapping in range(2):
        for head in range(heads):
            part = q_ref[:, head * 2 * HEAD : (head + 1) * 2 * HEAD] * HEAD ** (-0.5)
            keep = (lane < HEAD) if mapping == 0 else (lane >= HEAD)
            at = (mapping * heads + head) * rows
            wide_ref[at : at + rows, :] = jnp.where(keep, part, jnp.zeros_like(part))
    acc_ref[...] = jnp.zeros_like(acc_ref)
    stat_ref[...] = jnp.zeros_like(stat_ref)
    stat_ref[0:1, :] = jnp.full((1, stat_ref.shape[1]), -1e30, f32)
    count, cols = kv_ref.shape[0], 256
    key_at = lax.broadcasted_iota(jnp.int32, (count, cols), 0)
    query_at = lax.broadcasted_iota(jnp.int32, (count, cols), 1) % rows
    own_y = index_ref[0] % NY
    mask = key_at <= jnp.where(key_at < rows, query_at, own_y * rows + rows - 1)
    attend_block(kv_ref[...], wide_ref, acc_ref, stat_ref, mask, cols)


def more_kernel(index_ref, q_ref, *refs, steps):
    blocks, (acc_in, stat_in, acc_ref, stat_ref) = refs[: len(steps)], refs[len(steps) :]
    acc_ref[...] = acc_in[...]
    stat_ref[...] = stat_in[...]
    own_z = index_ref[0] // NY
    for step, block in zip(steps, blocks):
        needed = (own_z >= step) if step > 0 else (own_z - step >= NZ)

        @pl.when(needed)
        def _():
            attend_block(block[...], q_ref, acc_ref, stat_ref, None, 256)


SMEM = pl.BlockSpec(memory_space=pltpu.SMEM)
PARAMS = pltpu.CompilerParams(vmem_limit_bytes=16 << 20)
VMEM = pl.BlockSpec(memory_space=pltpu.VMEM)


def attend_first(index, queries, block):
    rows, heads = queries.shape[0], queries.shape[1] // (2 * HEAD)
    wide = 2 * heads * rows
    return pl.pallas_call(
        first_kernel,
        out_shape=(
            jax.ShapeDtypeStruct((wide, 2 * HEAD), bf16),
            jax.ShapeDtypeStruct((DV, wide), f32),
            jax.ShapeDtypeStruct((8, wide), f32),
        ),
        in_specs=[SMEM, VMEM, VMEM],
        out_specs=(VMEM, VMEM, VMEM),
        compiler_params=PARAMS,
        name="attend_first",
        cost_estimate=pl.CostEstimate(flops=4 << 30, bytes_accessed=1 << 20, transcendentals=0),
    )(index, queries, block)


def attend_more(index, wide, blocks, steps, state):
    acc, stat = state
    n = len(blocks)
    return pl.pallas_call(
        functools.partial(more_kernel, steps=steps),
        out_shape=(
            jax.ShapeDtypeStruct(acc.shape, f32),
            jax.ShapeDtypeStruct(stat.shape, f32),
        ),
        in_specs=[SMEM] + [VMEM] * (n + 3),
        out_specs=(VMEM, VMEM),
        input_output_aliases={2 + n: 0, 3 + n: 1},
        compiler_params=PARAMS,
        name="attend_more",
        cost_estimate=pl.CostEstimate(flops=4 << 30, bytes_accessed=1 << 20, transcendentals=0),
    )(index, wide, *blocks, acc, stat)


def last_kernel(
    index_ref, lambda_ref, gain_ref, acc_ref, stat_ref, recur_ref, w_ref, keep_ref, send_ref
):
    rows = recur_ref.shape[0]
    heads = acc_ref.shape[1] // (2 * rows)
    total = recur_ref[...]
    inverse = 1.0 / stat_ref[1:2, :]
    for head in range(heads):
        one = slice(head * rows, (head + 1) * rows)
        two = slice((heads + head) * rows, (heads + head + 1) * rows)
        out = acc_ref[:, one] * inverse[:, one] - lambda_ref[head] * (
            acc_ref[:, two] * inverse[:, two]
        )
        mean = jnp.mean(out * out, axis=0, keepdims=True)
        normed = (out * lax.rsqrt(mean + norm_eps) * gain_ref[...]).astype(bf16)
        total = total + jnp.dot(
            normed.T, w_ref[head * DV : (head + 1) * DV, :], preferred_element_type=f32
        )
    keep_low = index_ref[1] == 0
    half = rows // 2
    keep_ref[...] = jnp.where(keep_low, total[:half], total[half:])
    send_ref[...] = jnp.where(keep_low, total[half:], total[:half]).astype(bf16)


def last_part(index, lambdas, gain, state, recur, weight):
    acc, stat = state
    rows, cols = recur.shape
    return pl.pallas_call(
        last_kernel,
        out_shape=(
            jax.ShapeDtypeStruct((rows // 2, cols), f32),
            jax.ShapeDtypeStruct((rows // 2, cols), bf16),
        ),
        in_specs=[SMEM, SMEM] + [VMEM] * 5,
        out_specs=(VMEM, VMEM),
        compiler_params=PARAMS,
        name="last_part",
        cost_estimate=pl.CostEstimate(flops=4 << 30, bytes_accessed=4 << 20, transcendentals=0),
    )(index, lambdas, gain, acc, stat, recur, weight)


def norm_kernel(keep_ref, got_ref, gain_ref, out_ref):
    merged = keep_ref[...] + got_ref[...].astype(f32)
    mean = jnp.mean(merged * merged, axis=1, keepdims=True)
    out_ref[...] = (merged * lax.rsqrt(mean + norm_eps) * gain_ref[...]).astype(bf16)


def final_norm(keep, got, gain):
    return pl.pallas_call(
        norm_kernel,
        out_shape=jax.ShapeDtypeStruct(keep.shape, bf16),
        in_specs=[VMEM] * 3,
        out_specs=VMEM,
        compiler_params=PARAMS,
        name="final_norm",
    )(keep, got, gain)


def negative_expm1(y):
    series = 1.0 + y * (1.0 / 8.0)
    for k in (7, 6, 5, 4, 3, 2):
        series = 1.0 + y * (1.0 / k) * series
    return jnp.where(y > -0.5, -y * series, 1.0 - jnp.exp(y))


def recur_kernel(
    recur_ref,
    halo_ref,
    taps_ref,
    decay_w_ref,
    input_w_ref,
    base_ref,
    extra_ref,
    cum_ref,
    state_ref,
    total_ref,
    padded_ref,
):
    rows, cols = recur_ref.shape
    taps = taps_ref.shape[0]
    padded_ref[8 - (taps - 1) : 8, :] = halo_ref[...].astype(f32)
    padded_ref[8 : 8 + rows, :] = recur_ref[...].astype(f32)
    row = lax.broadcasted_iota(jnp.int32, (rows, 128), 0)
    low = lax.broadcasted_iota(jnp.int32, (rows, 128), 1) < HEAD
    square = lax.broadcasted_iota(jnp.int32, (128, 128), 0) < HEAD
    same = square == (lax.broadcasted_iota(jnp.int32, (128, 128), 1) < HEAD)
    for pair in range(cols // 128):
        lanes = slice(pair * 128, (pair + 1) * 128)
        conv = jnp.zeros((rows, 128), f32)
        for tap in range(taps):
            begin = 8 - (taps - 1) + tap
            conv = conv + taps_ref[tap : tap + 1, lanes] * padded_ref[begin : begin + rows, lanes]
        conv_in = conv.astype(bf16)

        def gate(w_ref):
            both = jnp.concatenate([w_ref[2 * pair], w_ref[2 * pair + 1]], axis=0)
            both = jnp.concatenate([both, both], axis=1)
            both = jnp.where(same, both, jnp.zeros_like(both))
            return jax.nn.sigmoid(jnp.dot(conv_in, both, preferred_element_type=f32))

        decay_gate = gate(decay_w_ref)
        input_gate = gate(input_w_ref)
        extra = jnp.where(
            low, extra_ref[:, 2 * pair : 2 * pair + 1], extra_ref[:, 2 * pair + 1 : 2 * pair + 2]
        )
        log_decay = -lru_rate * decay_gate * base_ref[:, lanes] - extra
        decay = jnp.exp(log_decay)
        inject = jnp.sqrt(negative_expm1(2.0 * log_decay)) * input_gate * conv_in.astype(f32)
        step = 1
        while step < rows:
            if step < 8:
                keep = row >= step
                decay_before = jnp.where(keep, pltpu.roll(decay, step, 0), 1.0)
                inject_before = jnp.where(keep, pltpu.roll(inject, step, 0), 0.0)
            else:
                one = jnp.ones((step, 128), f32)
                decay_before = jnp.concatenate([one, decay[:-step]], axis=0)
                inject_before = jnp.concatenate([jnp.zeros_like(one), inject[:-step]], axis=0)
            inject = inject + decay * inject_before
            decay = decay * decay_before
            step *= 2
        cum_ref[:, lanes] = decay
        state_ref[:, lanes] = inject
        total_ref[0:1, lanes] = decay[rows - 1 :]
        total_ref[1:2, lanes] = inject[rows - 1 :]


def recur_local(recur_in, halo, taps, decay_w, input_w, base, extra):
    rows, cols = recur_in.shape
    whole = jax.ShapeDtypeStruct((rows, cols), f32)
    return pl.pallas_call(
        recur_kernel,
        out_shape=(whole, whole, jax.ShapeDtypeStruct((2, cols), f32)),
        in_specs=[VMEM] * 7,
        out_specs=(VMEM,) * 3,
        scratch_shapes=[pltpu.VMEM((rows + 8, cols), f32)],
        compiler_params=PARAMS,
        name="recur_local",
        cost_estimate=pl.CostEstimate(flops=4 << 30, bytes_accessed=1 << 20, transcendentals=0),
    )(recur_in, halo, taps, decay_w, input_w, base, extra)


def join_kernel(index_ref, other_ref, group_ref, before_ref, group_out, before_out, *, bit):
    upper = (index_ref[0] & bit) != 0
    other, group = other_ref[...], group_ref[...]
    low = jnp.where(upper, other, group)
    high = jnp.where(upper, group, other)
    group_out[0:1, :] = low[0:1] * high[0:1]
    group_out[1:2, :] = high[0:1] * low[1:2] + high[1:2]
    before = before_ref[...]
    joined_decay = other[0:1] * before[0:1]
    joined_state = before[0:1] * other[1:2] + before[1:2]
    before_out[0:1, :] = jnp.where(upper, joined_decay, before[0:1])
    before_out[1:2, :] = jnp.where(upper, joined_state, before[1:2])


def join(index, other, group, before, bit):
    shape = jax.ShapeDtypeStruct(group.shape, f32)
    return pl.pallas_call(
        functools.partial(join_kernel, bit=bit),
        out_shape=(shape, shape),
        in_specs=[SMEM] + [VMEM] * 3,
        out_specs=(VMEM, VMEM),
        compiler_params=PARAMS,
        name="join",
    )(index, other, group, before)


def recur_out_kernel(state_ref, cum_ref, before_ref, w_ref, out_ref):
    out = (state_ref[...] + cum_ref[...] * before_ref[1:2, :]).astype(bf16)
    out_ref[...] = jnp.dot(out, w_ref[...], preferred_element_type=f32)


def recur_part(state, cum, before, weight):
    return pl.pallas_call(
        recur_out_kernel,
        out_shape=jax.ShapeDtypeStruct((state.shape[0], weight.shape[1]), f32),
        in_specs=[VMEM] * 4,
        out_specs=VMEM,
        compiler_params=PARAMS,
        name="recur_part",
        cost_estimate=pl.CostEstimate(flops=2 << 30, bytes_accessed=4 << 20, transcendentals=0),
    )(state, cum, before, weight)


def body(
    tokens,
    norm_gain,
    w_recur_in,
    conv_weight,
    w_gate_decay,
    w_gate_input,
    decay_base,
    extra_decay,
    w_query,
    w_key,
    w_value,
    mix_lambda,
    head_gain,
    w_out_recur,
    w_out_attend,
    out_gain,
):
    sp = lax.axis_index("sp").astype(jnp.int32)
    tp = lax.axis_index("tp").astype(jnp.int32)
    index = jnp.stack([sp, tp])
    row_count = tokens.shape[0]
    recur_cols = w_recur_in.shape[1]
    wide_piece = lax.all_gather(tokens, "tp", axis=1, tiled=True).astype(f32)
    scaled = (wide_piece * norm_gain).astype(bf16)
    squares = jnp.sum(wide_piece * wide_piece, axis=1, keepdims=True)
    inverse = lax.rsqrt(squares / D + norm_eps)

    def project(scaled, *weights):
        weight = jnp.concatenate(weights, axis=1)
        accum = jnp.dot(scaled, weight, preferred_element_type=f32)
        return (accum * inverse).astype(bf16)

    own = project(scaled, w_key, w_value)
    scaled = after(scaled, own)
    rest = project(scaled, w_recur_in, w_query)
    recur_in, queries = rest[:, :recur_cols], rest[:, recur_cols:]

    pieces = [own] + [lax.ppermute(own, "sp", sp_pairs(0, r)) for r in (1, 2, 3)]
    block = jnp.concatenate(pieces, axis=0)

    taps = conv_weight.shape[0]
    ends = [(i, i + 1) for i in range(NZ * NY - 1)]
    carried_rows = lax.ppermute(recur_in[row_count - (taps - 1) :], "sp", ends)
    cum, local_state, group = recur_local(
        recur_in,
        carried_rows,
        conv_weight,
        w_gate_decay,
        w_gate_input,
        decay_base[None, :],
        extra_decay,
    )
    before = jnp.stack([jnp.ones((recur_cols,), f32), jnp.zeros((recur_cols,), f32)])

    wide, acc, stat = attend_first(index, queries, block)
    state = (acc, stat)
    up = down = block
    bits = {2: (1, 2), 3: (4, 8), 4: (16,)}
    for step in range(1, NZ // 2 + 1):
        up = lax.ppermute(up, "sp", sp_pairs(1, 0))
        if step < NZ // 2:
            down = lax.ppermute(down, "sp", sp_pairs(-1, 0))
            state = attend_more(index, wide, (up, down), (step, -step), state)
        else:
            recur = recur_part(local_state, cum, before, w_out_recur)
            state = attend_more(index, wide, (up,), (step,), state)
        group = after(group, state[1])
        for bit in bits.get(step + 1, ()):
            other = lax.ppermute(group, "sp", xor_pairs(bit))
            group, before = join(index, other, group, before, bit)

    keep, send = last_part(index, mix_lambda, head_gain[:, None], state, recur, w_out_attend)
    got = lax.ppermute(send, "tp", [(0, 1), (1, 0)])
    return final_norm(keep, got, out_gain[None, :])


def solution(mesh):
    in_specs = (
        P(("fs", "sp"), "tp"),
        P(),
        P(None, "tp"),
        P(None, "tp"),
        P("tp", None, None),
        P("tp", None, None),
        P("tp"),
        P(("fs", "sp"), "tp"),
        P(None, "tp"),
        P(None, "tp"),
        P(None, "tp"),
        P("tp"),
        P(),
        P("tp", None),
        P("tp", None),
        P(),
    )
    out_specs = P(("fs", "sp", "tp"), None)
    return jax.shard_map(body, mesh=mesh, in_specs=in_specs, out_specs=out_specs, check_vma=False)
```

```python
import functools

import jax
import jax.numpy as jnp
from jax import lax
from jax.experimental import pallas as pl
from jax.experimental.pallas import tpu as pltpu
from jax.sharding import PartitionSpec as P

D = 2048
HEAD = 64
DV = 128
NY = 4
NZ = 8
lru_rate = 8.0
norm_eps = 1e-06
COLS = 128
EXTRA = 16
f32 = jnp.float32
bf16 = jnp.bfloat16


def sp_pairs(dz, dy):
    return [
        (z * NY + y, (z + dz) % NZ * NY + (y + dy) % NY) for z in range(NZ) for y in range(NY)
    ]


def xor_pairs(bit):
    return [(i, i ^ bit) for i in range(NZ * NY)]


def later(flip):
    return [(2 * i + t, 2 * i + 2 + (t ^ flip)) for i in range(NZ * NY - 1) for t in range(2)]


def after(value, other):
    return lax.optimization_barrier((value, other))[0]


def attend_block(kv, q_ref, acc_ref, stat_ref, score_ref, expo_ref, mask=None):
    keys = kv[:, : 2 * HEAD]
    values_t = kv[:, 2 * HEAD :].T
    cols = score_ref.shape[2]
    steps = q_ref.shape[0] // cols

    def score(i):
        score_ref[i % 2] = lax.dot_general(
            keys,
            q_ref[i * cols : (i + 1) * cols, :],
            (((1,), (1,)), ((), ())),
            preferred_element_type=f32,
        )

    def soften(i):
        part = slice(i * cols, (i + 1) * cols)
        scores = score_ref[i % 2]
        if mask is not None:
            scores = jnp.where(mask, scores, -1e30)
        old = stat_ref[0:1, part]
        peak = jnp.maximum(old, jnp.max(scores, axis=0, keepdims=True))
        fix = jnp.exp(old - peak)
        expo = jnp.exp(scores - peak)
        stat_ref[0:1, part] = peak
        stat_ref[1:2, part] = stat_ref[1:2, part] * fix + jnp.sum(expo, axis=0, keepdims=True)
        expo_ref[i % 2] = expo.astype(bf16)
        acc_ref[:, part] = acc_ref[:, part] * fix

    def gain(i):
        part = slice(i * cols, (i + 1) * cols)
        acc_ref[:, part] += jnp.dot(values_t, expo_ref[i % 2], preferred_element_type=f32)

    score(0)
    for i in range(steps):
        if i + 1 < steps:
            score(i + 1)
        soften(i)
        if i > 0:
            gain(i - 1)
    gain(steps - 1)


def attend_scratch(keys):
    return [pltpu.VMEM((2, keys, COLS), f32), pltpu.VMEM((2, keys, COLS), bf16)]


def first_kernel(wide_ref, block_ref, acc_ref, stat_ref, score_ref, expo_ref):
    rows = wide_ref.shape[0] // 8
    acc_ref[...] = jnp.zeros_like(acc_ref)
    stat_ref[...] = jnp.zeros_like(stat_ref)
    stat_ref[0:1, :] = jnp.full((1, stat_ref.shape[1]), -1e30, f32)
    count, cols = NY * rows, COLS
    key_at = lax.broadcasted_iota(jnp.int32, (count, cols), 0)
    query_at = lax.broadcasted_iota(jnp.int32, (count, cols), 1) % rows
    own_y = lax.axis_index("sp") % NY
    mask = key_at <= jnp.where(key_at < rows, query_at, own_y * rows + rows - 1)
    attend_block(block_ref[:count, :], wide_ref, acc_ref, stat_ref, score_ref, expo_ref, mask)


def take_block(step, block_ref, wide_ref, acc_ref, stat_ref, carry_ref, score_ref, expo_ref):
    count = block_ref.shape[0] - EXTRA
    own_z = lax.axis_index("sp") // NY
    needed = (own_z >= step) if step > 0 else (own_z - step >= NZ)

    @pl.when(needed)
    def _():
        attend_block(block_ref[:count, :], wide_ref, acc_ref, stat_ref, score_ref, expo_ref)
        decay, state = unpacked(block_ref[count:, :])
        if step > 0:
            before = carry_ref[0:1, :]
            carry_ref[1:2, :] = before * state + carry_ref[1:2, :]
            carry_ref[0:1, :] = before * decay
        else:
            carry_ref[3:4, :] = decay * carry_ref[3:4, :] + state
            carry_ref[2:3, :] = decay * carry_ref[2:3, :]


def more_kernel(wide_ref, *refs, steps):
    n = len(steps)
    blocks, (acc_in, stat_in, carry_in) = refs[:n], refs[n : n + 3]
    acc_ref, stat_ref, carry_ref, score_ref, expo_ref = refs[n + 3 :]
    acc_ref[...] = acc_in[...]
    stat_ref[...] = stat_in[...]
    carry_ref[...] = carry_in[...]
    for step, block in zip(steps, blocks):
        take_block(step, block, wide_ref, acc_ref, stat_ref, carry_ref, score_ref, expo_ref)


SMEM = pl.BlockSpec(memory_space=pltpu.SMEM)
PARAMS = pltpu.CompilerParams(vmem_limit_bytes=16 << 20)
VMEM = pl.BlockSpec(memory_space=pltpu.VMEM)
ANY = pl.BlockSpec(memory_space=pltpu.HBM)


def attend_first(wide, block):
    return pl.pallas_call(
        first_kernel,
        out_shape=(
            jax.ShapeDtypeStruct((DV, wide.shape[0]), f32),
            jax.ShapeDtypeStruct((8, wide.shape[0]), f32),
        ),
        in_specs=[VMEM, VMEM],
        out_specs=(VMEM, VMEM),
        scratch_shapes=attend_scratch(block.shape[0] - EXTRA),
        compiler_params=PARAMS,
        name="attend_first",
        cost_estimate=pl.CostEstimate(flops=4 << 30, bytes_accessed=1 << 20, transcendentals=0),
    )(wide, block)


def attend_more(wide, blocks, steps, state):
    n = len(blocks)
    return pl.pallas_call(
        functools.partial(more_kernel, steps=steps),
        out_shape=tuple(jax.ShapeDtypeStruct(a.shape, f32) for a in state),
        in_specs=[VMEM] * (n + 4),
        out_specs=(VMEM,) * 3,
        input_output_aliases={1 + n: 0, 2 + n: 1, 3 + n: 2},
        scratch_shapes=attend_scratch(blocks[0].shape[0] - EXTRA),
        compiler_params=PARAMS,
        name="attend_more",
        cost_estimate=pl.CostEstimate(flops=4 << 30, bytes_accessed=1 << 20, transcendentals=0),
    )(wide, *blocks, *state)


def last_kernel(
    lambda_ref,
    gain_ref,
    wide_ref,
    block_ref,
    acc_in,
    stat_in,
    carry_in,
    cum_ref,
    local_ref,
    recur_w_ref,
    attend_w_ref,
    keep_ref,
    send_ref,
    acc_ref,
    stat_ref,
    carry_ref,
    score_ref,
    expo_ref,
    *,
    step,
):
    acc_ref[...] = acc_in[...]
    stat_ref[...] = stat_in[...]
    carry_ref[...] = carry_in[...]
    take_block(step, block_ref, wide_ref, acc_ref, stat_ref, carry_ref, score_ref, expo_ref)
    before = carry_ref[0:1, :] * carry_ref[3:4, :] + carry_ref[1:2, :]
    recur_out = (local_ref[...] + cum_ref[...] * before).astype(bf16)
    rows = recur_out.shape[0]
    heads = acc_ref.shape[1] // (2 * rows)
    inverse = 1.0 / stat_ref[1:2, :]
    attend_out = []
    for head in range(heads):
        one = slice(head * rows, (head + 1) * rows)
        two = slice((heads + head) * rows, (heads + head + 1) * rows)
        out = acc_ref[:, one] * inverse[:, one] - lambda_ref[head] * (
            acc_ref[:, two] * inverse[:, two]
        )
        mean = jnp.mean(out * out, axis=0, keepdims=True)
        attend_out.append(((out * lax.rsqrt(mean + norm_eps)).T * gain_ref[...]).astype(bf16))
    total = jnp.dot(recur_out, recur_w_ref[...], preferred_element_type=f32) + jnp.dot(
        jnp.concatenate(attend_out, axis=1), attend_w_ref[...], preferred_element_type=f32
    )
    keep_low = lax.axis_index("tp") == 0
    half = rows // 2
    keep_ref[...] = jnp.where(keep_low, total[:half], total[half:])
    send_ref[...] = jnp.where(keep_low, total[half:], total[:half]).astype(bf16)


def last_part(lambdas, gain, wide, block, step, state, cum, local, recur_w, attend_w):
    rows, cols = cum.shape[0], recur_w.shape[1]
    return pl.pallas_call(
        functools.partial(last_kernel, step=step),
        out_shape=(
            jax.ShapeDtypeStruct((rows // 2, cols), f32),
            jax.ShapeDtypeStruct((rows // 2, cols), bf16),
        ),
        in_specs=[SMEM] + [VMEM] * 10,
        out_specs=(VMEM, VMEM),
        scratch_shapes=[pltpu.VMEM(a.shape, f32) for a in state]
        + attend_scratch(block.shape[0] - EXTRA),
        compiler_params=PARAMS,
        name="last_part",
        cost_estimate=pl.CostEstimate(flops=4 << 30, bytes_accessed=4 << 20, transcendentals=0),
    )(lambdas, gain, wide, block, *state, cum, local, recur_w, attend_w)


def norm_kernel(keep_ref, got_ref, gain_ref, out_ref):
    merged = keep_ref[...] + got_ref[...].astype(f32)
    mean = jnp.mean(merged * merged, axis=1, keepdims=True)
    out_ref[...] = (merged * lax.rsqrt(mean + norm_eps) * gain_ref[...]).astype(bf16)


def final_norm(keep, got, gain):
    return pl.pallas_call(
        norm_kernel,
        out_shape=jax.ShapeDtypeStruct(keep.shape, bf16),
        in_specs=[VMEM] * 3,
        out_specs=VMEM,
        compiler_params=PARAMS,
        name="final_norm",
    )(keep, got, gain)


def negative_expm1(y):
    series = 1.0 + y * (1.0 / 8.0)
    for k in (7, 6, 5, 4, 3, 2):
        series = 1.0 + y * (1.0 / k) * series
    return jnp.where(y > -0.5, -y * series, 1.0 - jnp.exp(y))


def packed(value):
    rows = []
    for _ in range(3):
        term = value.astype(bf16).astype(f32)
        value = value - term
        rows += [term[:, :256], term[:, 256:]]
    return rows


def unpacked(rows):
    rows = rows.astype(f32)
    sums = []
    for at in (0, 6):
        halves = [
            rows[at + half : at + half + 1]
            + rows[at + half + 2 : at + half + 3]
            + rows[at + half + 4 : at + half + 5]
            for half in range(2)
        ]
        sums.append(jnp.concatenate(halves, axis=1))
    return sums


def written(decay, state):
    rows = packed(decay) + packed(state)
    rows += [jnp.zeros_like(rows[0])] * (EXTRA - len(rows))
    return jnp.concatenate(rows, axis=0).astype(bf16)


def in_hbm(*arrays):
    return [pltpu.with_memory_space_constraint(a, pltpu.HBM) for a in arrays]


def started(pairs, sems):
    copies = [pltpu.make_async_copy(src, dst, sems.at[i]) for i, (src, dst) in enumerate(pairs)]
    for copy in copies:
        copy.start()
    return copies


def own_kernel(
    tokens_ref, gain_ref, *refs
):
    weights, (acc_ref, square_ref, own_ref, other_ref, held_ref, gain_held, sems) = refs[:4], refs[4:]
    width = tokens_ref.shape[1]
    tp = lax.axis_index("tp")
    mine = pl.ds(pl.multiple_of(tp * width, width), width)
    theirs = pl.ds(pl.multiple_of((1 - tp) * width, width), width)
    pairs = [(tokens_ref, held_ref), (gain_ref, gain_held)]
    parts, at = [], 0
    for w_ref in weights:
        parts.append(slice(at, at + w_ref.shape[1]))
        at += w_ref.shape[1]
    pairs += [(w_ref.at[mine, :], own_ref.at[:, part]) for w_ref, part in zip(weights, parts)]
    pairs += [(w_ref.at[theirs, :], other_ref.at[:, part]) for w_ref, part in zip(weights, parts)]
    copies = started(pairs, sems)
    copies[0].wait()
    copies[1].wait()
    tokens = held_ref[...].astype(f32)
    scaled = (tokens * gain_held[:, mine]).astype(bf16)
    square_ref[...] = jnp.broadcast_to(
        jnp.sum(tokens * tokens, axis=1, keepdims=True), square_ref.shape
    )
    for copy, part in zip(copies[2:6], parts):
        copy.wait()
        acc_ref[:, part] = jnp.dot(scaled, own_ref[:, part], preferred_element_type=f32)
    for copy in copies[6:]:
        copy.wait()


def project_own(tokens, gain, *weights):
    rows, width = tokens.shape
    cols = sum(w.shape[1] for w in weights)
    half = jax.ShapeDtypeStruct((width, cols), bf16)
    return pl.pallas_call(
        own_kernel,
        out_shape=(
            jax.ShapeDtypeStruct((rows, cols), f32),
            jax.ShapeDtypeStruct((rows, 128), f32),
            half,
            half,
        ),
        in_specs=[ANY] * 6,
        out_specs=(VMEM,) * 4,
        scratch_shapes=[
            pltpu.VMEM(tokens.shape, bf16),
            pltpu.VMEM(gain.shape, f32),
            pltpu.SemaphoreType.DMA((10,)),
        ],
        compiler_params=PARAMS,
        name="project_own",
        cost_estimate=pl.CostEstimate(flops=2 << 30, bytes_accessed=4 << 20, transcendentals=0),
    )(*in_hbm(tokens, gain, *weights))


def front_kernel(
    acc_ref,
    square_ref,
    own_w_ref,
    other_w_ref,
    other_ref,
    halo_own_ref,
    halo_other_ref,
    gain_hbm,
    taps_hbm,
    decay_hbm,
    input_hbm,
    base_hbm,
    extra_hbm,
    piece_ref,
    wide_ref,
    cum_ref,
    state_ref,
    padded_ref,
    gain_ref,
    taps_ref,
    decay_w_ref,
    input_w_ref,
    base_ref,
    extra_ref,
    sems,
):
    rows, width = other_ref.shape
    cols = cum_ref.shape[1]
    taps = taps_ref.shape[0]
    copies = started(
        [
            (gain_hbm, gain_ref),
            (taps_hbm, taps_ref),
            (decay_hbm, decay_w_ref),
            (input_hbm, input_w_ref),
            (base_hbm, base_ref),
            (extra_hbm, extra_ref),
        ],
        sems,
    )
    tp = lax.axis_index("tp")
    mine = pl.ds(pl.multiple_of(tp * width, width), width)
    theirs = pl.ds(pl.multiple_of((1 - tp) * width, width), width)
    copies[0].wait()

    def scaled(tokens, part):
        return (tokens * gain_ref[:, part]).astype(bf16)

    other = other_ref[...].astype(f32)
    square = square_ref[:, 0:1] + jnp.sum(other * other, axis=1, keepdims=True)
    inverse = lax.rsqrt(square / D + norm_eps)
    scaled_other = scaled(other, theirs)

    def project(at, count):
        lanes = slice(at, at + count)
        part = jnp.dot(scaled_other, other_w_ref[:, lanes], preferred_element_type=f32)
        return (acc_ref[:, lanes] + part) * inverse

    halo_own, halo_other = halo_own_ref[...].astype(f32), halo_other_ref[...].astype(f32)
    square = jnp.sum(halo_own * halo_own, axis=1, keepdims=True) + jnp.sum(
        halo_other * halo_other, axis=1, keepdims=True
    )
    halo = jnp.dot(scaled(halo_own, mine), own_w_ref[:, :cols], preferred_element_type=f32)
    halo += jnp.dot(scaled(halo_other, theirs), other_w_ref[:, :cols], preferred_element_type=f32)
    halo = (halo * lax.rsqrt(square / D + norm_eps)).astype(bf16)
    padded_ref[0:8, :] = halo.astype(f32)
    padded_ref[8 : 8 + rows, :] = project(0, cols).astype(bf16).astype(f32)

    at = own_w_ref.shape[1] - 2 * HEAD - DV
    piece_ref[:rows, : 2 * HEAD] = project(at, 2 * HEAD).astype(bf16)
    piece_ref[:rows, 2 * HEAD :] = project(at + 2 * HEAD, DV).astype(bf16)

    queries = project(cols, at - cols).astype(bf16) * HEAD ** (-0.5)
    heads = queries.shape[1] // (2 * HEAD)
    first = lax.broadcasted_iota(jnp.int32, (rows, 2 * HEAD), 1) < HEAD
    for head in range(heads):
        part = queries[:, head * 2 * HEAD : (head + 1) * 2 * HEAD]
        zero = jnp.zeros_like(part)
        wide_ref[head * rows : (head + 1) * rows, :] = jnp.where(first, part, zero)
        begin = (heads + head) * rows
        wide_ref[begin : begin + rows, :] = jnp.where(first, zero, part)

    for copy in copies[1:]:
        copy.wait()
    extra_decay = extra_ref[...].T
    row = lax.broadcasted_iota(jnp.int32, (rows, 128), 0)
    low = lax.broadcasted_iota(jnp.int32, (rows, 128), 1) < HEAD
    square = lax.broadcasted_iota(jnp.int32, (128, 128), 0) < HEAD
    same = square == (lax.broadcasted_iota(jnp.int32, (128, 128), 1) < HEAD)
    totals = []
    for pair in range(cols // 128):
        lanes = slice(pair * 128, (pair + 1) * 128)
        conv = jnp.zeros((rows, 128), f32)
        for tap in range(taps):
            begin = 8 - (taps - 1) + tap
            conv = conv + taps_ref[tap : tap + 1, lanes] * padded_ref[begin : begin + rows, lanes]
        conv_in = conv.astype(bf16)

        def gate(w_ref):
            both = jnp.concatenate([w_ref[2 * pair], w_ref[2 * pair + 1]], axis=0)
            both = jnp.concatenate([both, both], axis=1)
            both = jnp.where(same, both, jnp.zeros_like(both))
            return jax.nn.sigmoid(jnp.dot(conv_in, both, preferred_element_type=f32))

        decay_gate = gate(decay_w_ref)
        input_gate = gate(input_w_ref)
        extra = jnp.where(
            low,
            extra_decay[:, 2 * pair : 2 * pair + 1],
            extra_decay[:, 2 * pair + 1 : 2 * pair + 2],
        )
        log_decay = -lru_rate * decay_gate * base_ref[:, lanes] - extra
        decay = jnp.exp(log_decay)
        inject = jnp.sqrt(negative_expm1(2.0 * log_decay)) * input_gate * conv_in.astype(f32)
        step = 1
        while step < rows:
            if step < 8:
                keep = row >= step
                decay_before = jnp.where(keep, pltpu.roll(decay, step, 0), 1.0)
                inject_before = jnp.where(keep, pltpu.roll(inject, step, 0), 0.0)
            else:
                one = jnp.ones((step, 128), f32)
                decay_before = jnp.concatenate([one, decay[:-step]], axis=0)
                inject_before = jnp.concatenate([jnp.zeros_like(one), inject[:-step]], axis=0)
            inject = inject + decay * inject_before
            decay = decay * decay_before
            step *= 2
        cum_ref[:, lanes] = decay
        state_ref[:, lanes] = inject
        totals.append((decay[rows - 1 :], inject[rows - 1 :]))
    decay, state = (jnp.concatenate(t, axis=1) for t in zip(*totals))
    piece_ref[rows:, :] = written(decay, state)


def front(own, other, halos, small, cols):
    rows = other.shape[0]
    queries = own[0].shape[1] - cols - 2 * HEAD - DV
    whole = jax.ShapeDtypeStruct((rows, cols), f32)
    return pl.pallas_call(
        front_kernel,
        out_shape=(
            jax.ShapeDtypeStruct((rows + EXTRA, 2 * HEAD + DV), bf16),
            jax.ShapeDtypeStruct((2 * rows * queries // (2 * HEAD), 2 * HEAD), bf16),
            whole,
            whole,
        ),
        in_specs=[VMEM] * 7 + [ANY] * 6,
        out_specs=(VMEM,) * 4,
        scratch_shapes=[pltpu.VMEM((rows + 8, cols), f32)]
        + [pltpu.VMEM(a.shape, a.dtype) for a in small]
        + [pltpu.SemaphoreType.DMA((6,))],
        compiler_params=PARAMS,
        name="front",
        cost_estimate=pl.CostEstimate(flops=4 << 30, bytes_accessed=1 << 20, transcendentals=0),
    )(*own, other, *halos, *in_hbm(*small))


def assemble_kernel(*refs):
    pieces, (block_ref, carry_ref, each_ref) = refs[:NY], refs[NY:]
    rows = pieces[0].shape[0] - EXTRA
    for r, piece in enumerate(pieces):
        block_ref[r * rows : (r + 1) * rows, :] = piece[:rows, :]
        decay, state = unpacked(piece[rows:, :])
        each_ref[r, 0:1, :] = decay
        each_ref[r, 1:2, :] = state
    own_y = lax.axis_index("sp") % NY
    decay, state = each_ref[own_y, 0:1, :], each_ref[own_y, 1:2, :]
    before = [jnp.ones_like(decay), jnp.zeros_like(state)]
    for y in range(1, NY):
        earlier = y - 1 < own_y
        before = [
            jnp.where(earlier, decay, before[0]),
            jnp.where(earlier, state, before[1]),
        ]
        earlier = y <= own_y
        at = lax.rem(own_y - y + NY, NY)
        this = each_ref[at, 0:1, :]
        state = this * state + each_ref[at, 1:2, :]
        decay = this * decay
    block_ref[NY * rows :, :] = written(decay, state)
    carry_ref[...] = jnp.zeros_like(carry_ref)
    carry_ref[0:1, :] = before[0]
    carry_ref[1:2, :] = before[1]
    carry_ref[2:3, :] = jnp.ones_like(decay)


def assemble(pieces, cols):
    rows, width = pieces[0].shape
    return pl.pallas_call(
        assemble_kernel,
        out_shape=(
            jax.ShapeDtypeStruct((NY * (rows - EXTRA) + EXTRA, width), bf16),
            jax.ShapeDtypeStruct((8, cols), f32),
        ),
        in_specs=[VMEM] * NY,
        out_specs=(VMEM, VMEM),
        scratch_shapes=[pltpu.VMEM((NY, 8, cols), f32)],
        compiler_params=PARAMS,
        name="assemble",
    )(*pieces)


def body(
    tokens,
    norm_gain,
    w_recur_in,
    conv_weight,
    w_gate_decay,
    w_gate_input,
    decay_base,
    extra_decay,
    w_query,
    w_key,
    w_value,
    mix_lambda,
    head_gain,
    w_out_recur,
    w_out_attend,
    out_gain,
):
    rows = tokens.shape[0]
    recur_cols = w_recur_in.shape[1]
    weights = (w_recur_in, w_query, w_key, w_value)
    gain = norm_gain[None, :]

    swap = [(0, 1), (1, 0)]
    other = lax.ppermute(tokens, "tp", swap)
    ends = tokens[rows - 8 :]
    halo_own = lax.ppermute(ends, ("sp", "tp"), later(0))
    halo_other = lax.ppermute(ends, ("sp", "tp"), later(1))
    own = project_own(tokens, gain, *weights)
    small = (gain, conv_weight, w_gate_decay, w_gate_input, decay_base[None, :], extra_decay.T)
    piece, wide, cum, local = front(own, other, (halo_own, halo_other), small, recur_cols)

    pieces = [piece] + [lax.ppermute(piece, "sp", sp_pairs(0, r)) for r in range(1, NY)]
    block, carry = assemble(pieces, recur_cols)

    state = (*attend_first(wide, block), carry)
    up = down = block
    for step in range(1, NZ // 2):
        up = lax.ppermute(up, "sp", sp_pairs(1, 0))
        down = lax.ppermute(down, "sp", sp_pairs(-1, 0))
        state = attend_more(wide, (up, down), (step, -step), state)
    up = lax.ppermute(up, "sp", sp_pairs(1, 0))
    keep, send = last_part(
        mix_lambda,
        head_gain[None, :],
        wide,
        up,
        NZ // 2,
        state,
        cum,
        local,
        w_out_recur,
        w_out_attend,
    )
    got = lax.ppermute(send, "tp", swap)
    return final_norm(keep, got, out_gain[None, :])


def solution(mesh):
    in_specs = (
        P(("fs", "sp"), "tp"),
        P(),
        P(None, "tp"),
        P(None, "tp"),
        P("tp", None, None),
        P("tp", None, None),
        P("tp"),
        P(("fs", "sp"), "tp"),
        P(None, "tp"),
        P(None, "tp"),
        P(None, "tp"),
        P("tp"),
        P(),
        P("tp", None),
        P("tp", None),
        P(),
    )
    out_specs = P(("fs", "sp", "tp"), None)
    return jax.shard_map(body, mesh=mesh, in_specs=in_specs, out_specs=out_specs, check_vma=False)
```

```python
import functools

import jax
import jax.numpy as jnp
from jax import lax
from jax.experimental import pallas as pl
from jax.experimental.pallas import tpu as pltpu
from jax.sharding import PartitionSpec as P

D = 2048
HEAD = 64
DV = 128
NY = 4
NZ = 8
lru_rate = 8.0
norm_eps = 1e-06
COLS = 128
EXTRA = 16
f32 = jnp.float32
bf16 = jnp.bfloat16


def sp_pairs(dz, dy):
    return [
        (z * NY + y, (z + dz) % NZ * NY + (y + dy) % NY) for z in range(NZ) for y in range(NY)
    ]


def xor_pairs(bit):
    return [(i, i ^ bit) for i in range(NZ * NY)]


def later(flip):
    return [(2 * i + t, 2 * i + 2 + (t ^ flip)) for i in range(NZ * NY - 1) for t in range(2)]


def after(value, other):
    return lax.optimization_barrier((value, other))[0]


def attend_block(kv, q_ref, acc_ref, stat_ref, score_ref, expo_ref, mask=None):
    keys = kv[:, : 2 * HEAD]
    values_t = kv[:, 2 * HEAD :].T
    cols = score_ref.shape[2]
    steps = q_ref.shape[0] // cols

    def score(i):
        score_ref[i % 2] = lax.dot_general(
            keys,
            q_ref[i * cols : (i + 1) * cols, :],
            (((1,), (1,)), ((), ())),
            preferred_element_type=f32,
        )

    def soften(i):
        part = slice(i * cols, (i + 1) * cols)
        scores = score_ref[i % 2]
        if mask is not None:
            scores = jnp.where(mask, scores, -1e30)
        old = stat_ref[0:1, part]
        peak = jnp.maximum(old, jnp.max(scores, axis=0, keepdims=True))
        fix = jnp.exp(old - peak)
        expo = jnp.exp(scores - peak)
        stat_ref[0:1, part] = peak
        stat_ref[1:2, part] = stat_ref[1:2, part] * fix + jnp.sum(expo, axis=0, keepdims=True)
        expo_ref[i % 2] = expo.astype(bf16)
        acc_ref[:, part] = acc_ref[:, part] * fix

    def gain(i):
        part = slice(i * cols, (i + 1) * cols)
        acc_ref[:, part] += jnp.dot(values_t, expo_ref[i % 2], preferred_element_type=f32)

    score(0)
    for i in range(steps):
        if i + 1 < steps:
            score(i + 1)
        soften(i)
        if i > 0:
            gain(i - 1)
    gain(steps - 1)


def attend_scratch(keys):
    return [pltpu.VMEM((2, keys, COLS), f32), pltpu.VMEM((2, keys, COLS), bf16)]


def first_kernel(wide_ref, one_ref, two_ref, acc_ref, stat_ref, score_ref, expo_ref):
    rows = wide_ref.shape[0] // 8
    acc_ref[...] = jnp.zeros_like(acc_ref)
    stat_ref[...] = jnp.zeros_like(stat_ref)
    stat_ref[0:1, :] = jnp.full((1, stat_ref.shape[1]), -1e30, f32)
    count, cols = NY * rows, COLS
    key_at = lax.broadcasted_iota(jnp.int32, (count, cols), 0)
    query_at = lax.broadcasted_iota(jnp.int32, (count, cols), 1) % rows
    own_y = lax.axis_index("sp") % NY
    mask = key_at <= jnp.where(key_at < rows, query_at, own_y * rows + rows - 1)
    block = jnp.concatenate([one_ref[: count // 2, :], two_ref[...]], axis=0)
    attend_block(block, wide_ref, acc_ref, stat_ref, score_ref, expo_ref, mask)


def take_block(step, halves, wide_ref, acc_ref, stat_ref, carry_ref, score_ref, expo_ref):
    one_ref, two_ref = halves
    count = two_ref.shape[0]
    own_z = lax.axis_index("sp") // NY
    needed = (own_z >= step) if step > 0 else (own_z - step >= NZ)

    @pl.when(needed)
    def _():
        block = jnp.concatenate([one_ref[:count, :], two_ref[...]], axis=0)
        attend_block(block, wide_ref, acc_ref, stat_ref, score_ref, expo_ref)
        decay, state = unpacked(one_ref[count:, :])
        if step > 0:
            before = carry_ref[0:1, :]
            carry_ref[1:2, :] = before * state + carry_ref[1:2, :]
            carry_ref[0:1, :] = before * decay
        else:
            carry_ref[3:4, :] = decay * carry_ref[3:4, :] + state
            carry_ref[2:3, :] = decay * carry_ref[2:3, :]


def more_kernel(wide_ref, *refs, steps):
    n = 2 * len(steps)
    blocks, (acc_in, stat_in, carry_in) = refs[:n], refs[n : n + 3]
    acc_ref, stat_ref, carry_ref, score_ref, expo_ref = refs[n + 3 :]
    acc_ref[...] = acc_in[...]
    stat_ref[...] = stat_in[...]
    carry_ref[...] = carry_in[...]
    for step, block in zip(steps, zip(blocks[::2], blocks[1::2])):
        take_block(step, block, wide_ref, acc_ref, stat_ref, carry_ref, score_ref, expo_ref)


SMEM = pl.BlockSpec(memory_space=pltpu.SMEM)
PARAMS = pltpu.CompilerParams(vmem_limit_bytes=16 << 20)
VMEM = pl.BlockSpec(memory_space=pltpu.VMEM)
ANY = pl.BlockSpec(memory_space=pltpu.HBM)


def attend_first(wide, one, two):
    return pl.pallas_call(
        first_kernel,
        out_shape=(
            jax.ShapeDtypeStruct((DV, wide.shape[0]), f32),
            jax.ShapeDtypeStruct((8, wide.shape[0]), f32),
        ),
        in_specs=[VMEM] * 3,
        out_specs=(VMEM, VMEM),
        scratch_shapes=attend_scratch(2 * two.shape[0]),
        compiler_params=PARAMS,
        name="attend_first",
        cost_estimate=pl.CostEstimate(flops=4 << 30, bytes_accessed=1 << 20, transcendentals=0),
    )(wide, one, two)


def attend_more(wide, blocks, steps, state):
    n = len(blocks)
    return pl.pallas_call(
        functools.partial(more_kernel, steps=steps),
        out_shape=tuple(jax.ShapeDtypeStruct(a.shape, f32) for a in state),
        in_specs=[VMEM] * (n + 4),
        out_specs=(VMEM,) * 3,
        input_output_aliases={1 + n: 0, 2 + n: 1, 3 + n: 2},
        scratch_shapes=attend_scratch(2 * blocks[1].shape[0]),
        compiler_params=PARAMS,
        name="attend_more",
        cost_estimate=pl.CostEstimate(flops=4 << 30, bytes_accessed=1 << 20, transcendentals=0),
    )(wide, *blocks, *state)


def last_kernel(
    lambda_ref,
    gain_ref,
    wide_ref,
    one_ref,
    two_ref,
    acc_in,
    stat_in,
    carry_in,
    cum_ref,
    local_ref,
    recur_w_ref,
    attend_w_ref,
    keep_ref,
    send_ref,
    acc_ref,
    stat_ref,
    carry_ref,
    score_ref,
    expo_ref,
    *,
    step,
):
    acc_ref[...] = acc_in[...]
    stat_ref[...] = stat_in[...]
    carry_ref[...] = carry_in[...]
    halves = (one_ref, two_ref)
    take_block(step, halves, wide_ref, acc_ref, stat_ref, carry_ref, score_ref, expo_ref)
    before = carry_ref[0:1, :] * carry_ref[3:4, :] + carry_ref[1:2, :]
    recur_out = (local_ref[...] + cum_ref[...] * before).astype(bf16)
    rows = recur_out.shape[0]
    heads = acc_ref.shape[1] // (2 * rows)
    inverse = 1.0 / stat_ref[1:2, :]
    attend_out = []
    for head in range(heads):
        one = slice(head * rows, (head + 1) * rows)
        two = slice((heads + head) * rows, (heads + head + 1) * rows)
        out = acc_ref[:, one] * inverse[:, one] - lambda_ref[head] * (
            acc_ref[:, two] * inverse[:, two]
        )
        mean = jnp.mean(out * out, axis=0, keepdims=True)
        attend_out.append(((out * lax.rsqrt(mean + norm_eps)).T * gain_ref[...]).astype(bf16))
    total = jnp.dot(recur_out, recur_w_ref[...], preferred_element_type=f32) + jnp.dot(
        jnp.concatenate(attend_out, axis=1), attend_w_ref[...], preferred_element_type=f32
    )
    keep_low = lax.axis_index("tp") == 0
    half = rows // 2
    keep_ref[...] = jnp.where(keep_low, total[:half], total[half:])
    send_ref[...] = jnp.where(keep_low, total[half:], total[:half]).astype(bf16)


def last_part(lambdas, gain, wide, one, two, step, state, cum, local, recur_w, attend_w):
    rows, cols = cum.shape[0], recur_w.shape[1]
    return pl.pallas_call(
        functools.partial(last_kernel, step=step),
        out_shape=(
            jax.ShapeDtypeStruct((rows // 2, cols), f32),
            jax.ShapeDtypeStruct((rows // 2, cols), bf16),
        ),
        in_specs=[SMEM] + [VMEM] * 11,
        out_specs=(VMEM, VMEM),
        scratch_shapes=[pltpu.VMEM(a.shape, f32) for a in state]
        + attend_scratch(2 * two.shape[0]),
        compiler_params=PARAMS,
        name="last_part",
        cost_estimate=pl.CostEstimate(flops=4 << 30, bytes_accessed=4 << 20, transcendentals=0),
    )(lambdas, gain, wide, one, two, *state, cum, local, recur_w, attend_w)


def norm_kernel(keep_ref, got_ref, gain_ref, out_ref):
    merged = keep_ref[...] + got_ref[...].astype(f32)
    mean = jnp.mean(merged * merged, axis=1, keepdims=True)
    out_ref[...] = (merged * lax.rsqrt(mean + norm_eps) * gain_ref[...]).astype(bf16)


def final_norm(keep, got, gain):
    return pl.pallas_call(
        norm_kernel,
        out_shape=jax.ShapeDtypeStruct(keep.shape, bf16),
        in_specs=[VMEM] * 3,
        out_specs=VMEM,
        compiler_params=PARAMS,
        name="final_norm",
    )(keep, got, gain)


def negative_expm1(y):
    series = 1.0 + y * (1.0 / 8.0)
    for k in (7, 6, 5, 4, 3, 2):
        series = 1.0 + y * (1.0 / k) * series
    return jnp.where(y > -0.5, -y * series, 1.0 - jnp.exp(y))


def packed(value):
    rows = []
    for _ in range(3):
        term = value.astype(bf16).astype(f32)
        value = value - term
        rows += [term[:, :256], term[:, 256:]]
    return rows


def unpacked(rows):
    rows = rows.astype(f32)
    sums = []
    for at in (0, 6):
        halves = [
            rows[at + half : at + half + 1]
            + rows[at + half + 2 : at + half + 3]
            + rows[at + half + 4 : at + half + 5]
            for half in range(2)
        ]
        sums.append(jnp.concatenate(halves, axis=1))
    return sums


def written(decay, state):
    rows = packed(decay) + packed(state)
    rows += [jnp.zeros_like(rows[0])] * (EXTRA - len(rows))
    return jnp.concatenate(rows, axis=0).astype(bf16)


def in_hbm(*arrays):
    return [pltpu.with_memory_space_constraint(a, pltpu.HBM) for a in arrays]


def started(pairs, sems):
    copies = [pltpu.make_async_copy(src, dst, sems.at[i]) for i, (src, dst) in enumerate(pairs)]
    for copy in copies:
        copy.start()
    return copies


def own_kernel(
    tokens_ref, gain_ref, *refs
):
    weights, (acc_ref, square_ref, own_ref, other_ref, held_ref, gain_held, sems) = refs[:4], refs[4:]
    width = tokens_ref.shape[1]
    tp = lax.axis_index("tp")
    mine = pl.ds(pl.multiple_of(tp * width, width), width)
    theirs = pl.ds(pl.multiple_of((1 - tp) * width, width), width)
    pairs = [(tokens_ref, held_ref), (gain_ref, gain_held)]
    parts, at = [], 0
    for w_ref in weights:
        parts.append(slice(at, at + w_ref.shape[1]))
        at += w_ref.shape[1]
    pairs += [(w_ref.at[mine, :], own_ref.at[:, part]) for w_ref, part in zip(weights, parts)]
    pairs += [(w_ref.at[theirs, :], other_ref.at[:, part]) for w_ref, part in zip(weights, parts)]
    copies = started(pairs, sems)
    copies[0].wait()
    copies[1].wait()
    tokens = held_ref[...].astype(f32)
    scaled = (tokens * gain_held[:, mine]).astype(bf16)
    square_ref[...] = jnp.broadcast_to(
        jnp.sum(tokens * tokens, axis=1, keepdims=True), square_ref.shape
    )
    for copy, part in zip(copies[2:6], parts):
        copy.wait()
        acc_ref[:, part] = jnp.dot(scaled, own_ref[:, part], preferred_element_type=f32)
    for copy in copies[6:]:
        copy.wait()


def project_own(tokens, gain, *weights):
    rows, width = tokens.shape
    cols = sum(w.shape[1] for w in weights)
    half = jax.ShapeDtypeStruct((width, cols), bf16)
    return pl.pallas_call(
        own_kernel,
        out_shape=(
            jax.ShapeDtypeStruct((rows, cols), f32),
            jax.ShapeDtypeStruct((rows, 128), f32),
            half,
            half,
        ),
        in_specs=[ANY] * 6,
        out_specs=(VMEM,) * 4,
        scratch_shapes=[
            pltpu.VMEM(tokens.shape, bf16),
            pltpu.VMEM(gain.shape, f32),
            pltpu.SemaphoreType.DMA((10,)),
        ],
        compiler_params=PARAMS,
        name="project_own",
        cost_estimate=pl.CostEstimate(flops=2 << 30, bytes_accessed=4 << 20, transcendentals=0),
    )(*in_hbm(tokens, gain, *weights))


def front_kernel(
    acc_ref,
    square_ref,
    own_w_ref,
    other_w_ref,
    other_ref,
    halo_own_ref,
    halo_other_ref,
    gain_hbm,
    taps_hbm,
    decay_hbm,
    input_hbm,
    base_hbm,
    extra_hbm,
    piece_ref,
    wide_ref,
    cum_ref,
    state_ref,
    padded_ref,
    gain_ref,
    taps_ref,
    decay_w_ref,
    input_w_ref,
    base_ref,
    extra_ref,
    sems,
):
    rows, width = other_ref.shape
    cols = cum_ref.shape[1]
    taps = taps_ref.shape[0]
    copies = started(
        [
            (gain_hbm, gain_ref),
            (taps_hbm, taps_ref),
            (decay_hbm, decay_w_ref),
            (input_hbm, input_w_ref),
            (base_hbm, base_ref),
            (extra_hbm, extra_ref),
        ],
        sems,
    )
    tp = lax.axis_index("tp")
    mine = pl.ds(pl.multiple_of(tp * width, width), width)
    theirs = pl.ds(pl.multiple_of((1 - tp) * width, width), width)
    copies[0].wait()

    def scaled(tokens, part):
        return (tokens * gain_ref[:, part]).astype(bf16)

    other = other_ref[...].astype(f32)
    square = square_ref[:, 0:1] + jnp.sum(other * other, axis=1, keepdims=True)
    inverse = lax.rsqrt(square / D + norm_eps)
    scaled_other = scaled(other, theirs)

    def project(at, count):
        lanes = slice(at, at + count)
        part = jnp.dot(scaled_other, other_w_ref[:, lanes], preferred_element_type=f32)
        return (acc_ref[:, lanes] + part) * inverse

    halo_own, halo_other = halo_own_ref[...].astype(f32), halo_other_ref[...].astype(f32)
    square = jnp.sum(halo_own * halo_own, axis=1, keepdims=True) + jnp.sum(
        halo_other * halo_other, axis=1, keepdims=True
    )
    halo = jnp.dot(scaled(halo_own, mine), own_w_ref[:, :cols], preferred_element_type=f32)
    halo += jnp.dot(scaled(halo_other, theirs), other_w_ref[:, :cols], preferred_element_type=f32)
    halo = (halo * lax.rsqrt(square / D + norm_eps)).astype(bf16)
    padded_ref[0:8, :] = halo.astype(f32)
    padded_ref[8 : 8 + rows, :] = project(0, cols).astype(bf16).astype(f32)

    at = own_w_ref.shape[1] - 2 * HEAD - DV
    piece_ref[:rows, : 2 * HEAD] = project(at, 2 * HEAD).astype(bf16)
    piece_ref[:rows, 2 * HEAD :] = project(at + 2 * HEAD, DV).astype(bf16)

    queries = project(cols, at - cols).astype(bf16) * HEAD ** (-0.5)
    heads = queries.shape[1] // (2 * HEAD)
    first = lax.broadcasted_iota(jnp.int32, (rows, 2 * HEAD), 1) < HEAD
    for head in range(heads):
        part = queries[:, head * 2 * HEAD : (head + 1) * 2 * HEAD]
        zero = jnp.zeros_like(part)
        wide_ref[head * rows : (head + 1) * rows, :] = jnp.where(first, part, zero)
        begin = (heads + head) * rows
        wide_ref[begin : begin + rows, :] = jnp.where(first, zero, part)

    for copy in copies[1:]:
        copy.wait()
    extra_decay = extra_ref[...].T
    row = lax.broadcasted_iota(jnp.int32, (rows, 128), 0)
    low = lax.broadcasted_iota(jnp.int32, (rows, 128), 1) < HEAD
    square = lax.broadcasted_iota(jnp.int32, (128, 128), 0) < HEAD
    same = square == (lax.broadcasted_iota(jnp.int32, (128, 128), 1) < HEAD)
    totals = []
    for pair in range(cols // 128):
        lanes = slice(pair * 128, (pair + 1) * 128)
        conv = jnp.zeros((rows, 128), f32)
        for tap in range(taps):
            begin = 8 - (taps - 1) + tap
            conv = conv + taps_ref[tap : tap + 1, lanes] * padded_ref[begin : begin + rows, lanes]
        conv_in = conv.astype(bf16)

        def gate(w_ref):
            both = jnp.concatenate([w_ref[2 * pair], w_ref[2 * pair + 1]], axis=0)
            both = jnp.concatenate([both, both], axis=1)
            both = jnp.where(same, both, jnp.zeros_like(both))
            return jax.nn.sigmoid(jnp.dot(conv_in, both, preferred_element_type=f32))

        decay_gate = gate(decay_w_ref)
        input_gate = gate(input_w_ref)
        extra = jnp.where(
            low,
            extra_decay[:, 2 * pair : 2 * pair + 1],
            extra_decay[:, 2 * pair + 1 : 2 * pair + 2],
        )
        log_decay = -lru_rate * decay_gate * base_ref[:, lanes] - extra
        decay = jnp.exp(log_decay)
        inject = jnp.sqrt(negative_expm1(2.0 * log_decay)) * input_gate * conv_in.astype(f32)
        step = 1
        while step < rows:
            if step < 8:
                keep = row >= step
                decay_before = jnp.where(keep, pltpu.roll(decay, step, 0), 1.0)
                inject_before = jnp.where(keep, pltpu.roll(inject, step, 0), 0.0)
            else:
                one = jnp.ones((step, 128), f32)
                decay_before = jnp.concatenate([one, decay[:-step]], axis=0)
                inject_before = jnp.concatenate([jnp.zeros_like(one), inject[:-step]], axis=0)
            inject = inject + decay * inject_before
            decay = decay * decay_before
            step *= 2
        cum_ref[:, lanes] = decay
        state_ref[:, lanes] = inject
        totals.append((decay[rows - 1 :], inject[rows - 1 :]))
    decay, state = (jnp.concatenate(t, axis=1) for t in zip(*totals))
    piece_ref[rows:, :] = written(decay, state)


def front(own, other, halos, small, cols):
    rows = other.shape[0]
    queries = own[0].shape[1] - cols - 2 * HEAD - DV
    whole = jax.ShapeDtypeStruct((rows, cols), f32)
    return pl.pallas_call(
        front_kernel,
        out_shape=(
            jax.ShapeDtypeStruct((rows + EXTRA, 2 * HEAD + DV), bf16),
            jax.ShapeDtypeStruct((2 * rows * queries // (2 * HEAD), 2 * HEAD), bf16),
            whole,
            whole,
        ),
        in_specs=[VMEM] * 7 + [ANY] * 6,
        out_specs=(VMEM,) * 4,
        scratch_shapes=[pltpu.VMEM((rows + 8, cols), f32)]
        + [pltpu.VMEM(a.shape, a.dtype) for a in small]
        + [pltpu.SemaphoreType.DMA((6,))],
        compiler_params=PARAMS,
        name="front",
        cost_estimate=pl.CostEstimate(flops=4 << 30, bytes_accessed=1 << 20, transcendentals=0),
    )(*own, other, *halos, *in_hbm(*small))


def assemble_kernel(*refs):
    pieces, (one_ref, two_ref, carry_ref, each_ref) = refs[:NY], refs[NY:]
    rows = pieces[0].shape[0] - EXTRA
    for r, piece in enumerate(pieces):
        half_ref, at = (one_ref, two_ref)[r // 2], r % 2 * rows
        half_ref[at : at + rows, :] = piece[:rows, :]
        decay, state = unpacked(piece[rows:, :])
        each_ref[r, 0:1, :] = decay
        each_ref[r, 1:2, :] = state
    own_y = lax.axis_index("sp") % NY
    decay, state = each_ref[own_y, 0:1, :], each_ref[own_y, 1:2, :]
    before = [jnp.ones_like(decay), jnp.zeros_like(state)]
    for y in range(1, NY):
        earlier = y - 1 < own_y
        before = [
            jnp.where(earlier, decay, before[0]),
            jnp.where(earlier, state, before[1]),
        ]
        earlier = y <= own_y
        at = lax.rem(own_y - y + NY, NY)
        this = each_ref[at, 0:1, :]
        state = this * state + each_ref[at, 1:2, :]
        decay = this * decay
    one_ref[NY // 2 * rows :, :] = written(decay, state)
    carry_ref[...] = jnp.zeros_like(carry_ref)
    carry_ref[0:1, :] = before[0]
    carry_ref[1:2, :] = before[1]
    carry_ref[2:3, :] = jnp.ones_like(decay)


def assemble(pieces, cols):
    rows, width = pieces[0].shape
    return pl.pallas_call(
        assemble_kernel,
        out_shape=(
            jax.ShapeDtypeStruct((NY // 2 * (rows - EXTRA) + EXTRA, width), bf16),
            jax.ShapeDtypeStruct((NY // 2 * (rows - EXTRA), width), bf16),
            jax.ShapeDtypeStruct((8, cols), f32),
        ),
        in_specs=[VMEM] * NY,
        out_specs=(VMEM,) * 3,
        scratch_shapes=[pltpu.VMEM((NY, 8, cols), f32)],
        compiler_params=PARAMS,
        name="assemble",
    )(*pieces)


def body(
    tokens,
    norm_gain,
    w_recur_in,
    conv_weight,
    w_gate_decay,
    w_gate_input,
    decay_base,
    extra_decay,
    w_query,
    w_key,
    w_value,
    mix_lambda,
    head_gain,
    w_out_recur,
    w_out_attend,
    out_gain,
):
    rows = tokens.shape[0]
    recur_cols = w_recur_in.shape[1]
    weights = (w_recur_in, w_query, w_key, w_value)
    gain = norm_gain[None, :]

    swap = [(0, 1), (1, 0)]
    other = lax.ppermute(tokens, "tp", swap)
    ends = tokens[rows - 8 :]
    halo_own = lax.ppermute(ends, ("sp", "tp"), later(0))
    halo_other = lax.ppermute(ends, ("sp", "tp"), later(1))
    own = project_own(tokens, gain, *weights)
    small = (gain, conv_weight, w_gate_decay, w_gate_input, decay_base[None, :], extra_decay.T)
    piece, wide, cum, local = front(own, other, (halo_own, halo_other), small, recur_cols)

    pieces = [piece] + [lax.ppermute(piece, "sp", sp_pairs(0, r)) for r in range(1, NY)]
    one, two, carry = assemble(pieces, recur_cols)

    state = (*attend_first(wide, one, two), carry)
    up, down = (one, two), (one, two)
    for step in range(1, NZ // 2):
        up = tuple(lax.ppermute(half, "sp", sp_pairs(1, 0)) for half in up)
        down = tuple(lax.ppermute(half, "sp", sp_pairs(-1, 0)) for half in down)
        state = attend_more(wide, (*up, *down), (step, -step), state)
    one = lax.ppermute(up[0], "sp", sp_pairs(1, 0))
    two = lax.ppermute(down[1], "sp", sp_pairs(-1, 0))
    keep, send = last_part(
        mix_lambda,
        head_gain[None, :],
        wide,
        one,
        two,
        NZ // 2,
        state,
        cum,
        local,
        w_out_recur,
        w_out_attend,
    )
    got = lax.ppermute(send, "tp", swap)
    return final_norm(keep, got, out_gain[None, :])


def solution(mesh):
    in_specs = (
        P(("fs", "sp"), "tp"),
        P(),
        P(None, "tp"),
        P(None, "tp"),
        P("tp", None, None),
        P("tp", None, None),
        P("tp"),
        P(("fs", "sp"), "tp"),
        P(None, "tp"),
        P(None, "tp"),
        P(None, "tp"),
        P("tp"),
        P(),
        P("tp", None),
        P("tp", None),
        P(),
    )
    out_specs = P(("fs", "sp", "tp"), None)
    return jax.shard_map(body, mesh=mesh, in_specs=in_specs, out_specs=out_specs, check_vma=False)
```

```python
import functools

import jax
import jax.numpy as jnp
from jax import lax
from jax.experimental import pallas as pl
from jax.experimental.pallas import tpu as pltpu
from jax.sharding import PartitionSpec as P


D = 2048
HEAD = 64
DV = 128
NY = 4
NZ = 8
lru_rate = 8.0
norm_eps = 1e-06
COLS = 128
EXTRA = 16
f32 = jnp.float32
bf16 = jnp.bfloat16


def sp_pairs(dz, dy):
    return [
        (z * NY + y, (z + dz) % NZ * NY + (y + dy) % NY) for z in range(NZ) for y in range(NY)
    ]


def around():
    return [
        (2 * i + t, 2 * ((z + 1 - 2 * t) % NZ * NY + y) + t)
        for i in range(NZ * NY)
        for z, y in [divmod(i, NY)]
        for t in range(2)
    ]


def later(flip):
    return [(2 * i + t, 2 * i + 2 + (t ^ flip)) for i in range(NZ * NY - 1) for t in range(2)]


def attend_block(kv, q_ref, acc_ref, stat_ref, score_ref, expo_ref, mask=None):
    keys = kv[:, : 2 * HEAD]
    values_t = kv[:, 2 * HEAD :].T
    cols = score_ref.shape[2]
    steps = q_ref.shape[0] // cols

    def score(i):
        score_ref[i % 2] = lax.dot_general(
            keys,
            q_ref[i * cols : (i + 1) * cols, :],
            (((1,), (1,)), ((), ())),
            preferred_element_type=f32,
        )

    def soften(i):
        part = slice(i * cols, (i + 1) * cols)
        scores = score_ref[i % 2]
        if mask is not None:
            scores = jnp.where(mask, scores, -1e30)
        old = stat_ref[0:1, part]
        peak = jnp.maximum(old, jnp.max(scores, axis=0, keepdims=True))
        fix = jnp.exp(old - peak)
        expo = jnp.exp(scores - peak)
        stat_ref[0:1, part] = peak
        stat_ref[1:2, part] = stat_ref[1:2, part] * fix + jnp.sum(expo, axis=0, keepdims=True)
        expo_ref[i % 2] = expo.astype(bf16)
        acc_ref[:, part] = acc_ref[:, part] * fix

    def gain(i):
        part = slice(i * cols, (i + 1) * cols)
        acc_ref[:, part] += jnp.dot(values_t, expo_ref[i % 2], preferred_element_type=f32)

    score(0)
    for i in range(steps):
        if i + 1 < steps:
            score(i + 1)
        soften(i)
        if i > 0:
            gain(i - 1)
    gain(steps - 1)


def attend_scratch(keys):
    return [pltpu.VMEM((2, keys, COLS), f32), pltpu.VMEM((2, keys, COLS), bf16)]


def first_kernel(
    wide_ref,
    block_ref,
    acc_ref,
    stat_ref,
    score_ref,
    expo_ref,
):
    rows = wide_ref.shape[0] // 8
    acc_ref[...] = jnp.zeros_like(acc_ref)
    stat_ref[...] = jnp.zeros_like(stat_ref)
    stat_ref[0:1, :] = jnp.full((1, stat_ref.shape[1]), -1e30, f32)
    count, cols = NY * rows, COLS
    key_at = lax.broadcasted_iota(jnp.int32, (count, cols), 0)
    query_at = lax.broadcasted_iota(jnp.int32, (count, cols), 1) % rows
    own_y = lax.axis_index("sp") % NY
    mask = key_at <= jnp.where(key_at < rows, query_at, own_y * rows + rows - 1)
    attend_block(block_ref[EXTRA:, :], wide_ref, acc_ref, stat_ref, score_ref, expo_ref, mask)


def take_block(step, up, parts, wide_ref, acc_ref, stat_ref, carry_ref, score_ref, expo_ref):
    own_z = lax.axis_index("sp") // NY
    needed = jnp.where(up, own_z, own_z + 2 * step - NZ) >= step

    @pl.when(needed)
    def _():
        block = jnp.concatenate([parts[0][EXTRA:, :]] + [part[...] for part in parts[1:]], axis=0)
        attend_block(block, wide_ref, acc_ref, stat_ref, score_ref, expo_ref)

    @pl.when(jnp.logical_and(needed, up))
    def _():
        decay, state = unpacked(parts[0][:EXTRA, :])
        before = carry_ref[0:1, :]
        carry_ref[1:2, :] = before * state + carry_ref[1:2, :]
        carry_ref[0:1, :] = before * decay

    @pl.when(jnp.logical_and(needed, jnp.logical_not(up)))
    def _():
        decay, state = unpacked(parts[0][:EXTRA, :])
        carry_ref[3:4, :] = decay * carry_ref[3:4, :] + state
        carry_ref[2:3, :] = decay * carry_ref[2:3, :]


def more_kernel(wide_ref, *refs, steps):
    n = sum(count for _, _, count in steps)
    blocks, (acc_in, stat_in, carry_in) = list(refs[:n]), refs[n : n + 3]
    acc_ref, stat_ref, carry_ref, score_ref, expo_ref = refs[n + 3 :]
    acc_ref[...] = acc_in[...]
    stat_ref[...] = stat_in[...]
    carry_ref[...] = carry_in[...]
    core = lax.axis_index("tp")
    refs = (wide_ref, acc_ref, stat_ref, carry_ref, score_ref, expo_ref)
    for step, up_core, count in steps:
        parts, blocks = blocks[:count], blocks[count:]
        take_block(step, core == up_core, parts, *refs)


SMEM = pl.BlockSpec(memory_space=pltpu.SMEM)
PARAMS = pltpu.CompilerParams(vmem_limit_bytes=16 << 20)
VMEM = pl.BlockSpec(memory_space=pltpu.VMEM)
ANY = pl.BlockSpec(memory_space=pltpu.HBM)


def attend_first(wide, block):
    return pl.pallas_call(
        first_kernel,
        out_shape=(
            jax.ShapeDtypeStruct((DV, wide.shape[0]), f32),
            jax.ShapeDtypeStruct((8, wide.shape[0]), f32),
        ),
        in_specs=[VMEM] * 2,
        out_specs=(VMEM,) * 2,
        scratch_shapes=attend_scratch(block.shape[0] - EXTRA),
        compiler_params=PARAMS,
        name="attend_first",
        cost_estimate=pl.CostEstimate(flops=4 << 30, bytes_accessed=1 << 20, transcendentals=0),
    )(wide, block)


def attend_more(wide, waiting, state):
    blocks = [part for parts, _, _ in waiting for part in parts]
    steps = tuple((step, up_core, len(parts)) for parts, step, up_core in waiting)
    n = len(blocks)
    return pl.pallas_call(
        functools.partial(more_kernel, steps=steps),
        out_shape=tuple(jax.ShapeDtypeStruct(a.shape, f32) for a in state),
        in_specs=[VMEM] * (n + 4),
        out_specs=(VMEM,) * 3,
        input_output_aliases={n + 1: 0, n + 2: 1, n + 3: 2},
        scratch_shapes=attend_scratch(sum(part.shape[0] for part in waiting[0][0]) - EXTRA),
        compiler_params=PARAMS,
        name="attend_more",
        cost_estimate=pl.CostEstimate(flops=4 << 30, bytes_accessed=1 << 20, transcendentals=0),
    )(wide, *blocks, *state)


def last_kernel(
    lambda_ref,
    gain_ref,
    wide_ref,
    one_ref,
    two_ref,
    acc_in,
    stat_in,
    carry_in,
    cum_ref,
    local_ref,
    recur_w_ref,
    attend_w_ref,
    keep_ref,
    send_ref,
    acc_ref,
    stat_ref,
    carry_ref,
    score_ref,
    expo_ref,
    *,
    step,
):
    acc_ref[...] = acc_in[...]
    stat_ref[...] = stat_in[...]
    carry_ref[...] = carry_in[...]
    refs = (wide_ref, acc_ref, stat_ref, carry_ref, score_ref, expo_ref)
    take_block(step, lax.axis_index("tp") >= 0, (one_ref, two_ref), *refs)
    before = carry_ref[0:1, :] * carry_ref[3:4, :] + carry_ref[1:2, :]
    recur_out = (local_ref[...] + cum_ref[...] * before).astype(bf16)
    rows = recur_out.shape[0]
    heads = acc_ref.shape[1] // (2 * rows)
    inverse = 1.0 / stat_ref[1:2, :]
    attend_out = []
    for head in range(heads):
        one = slice(head * rows, (head + 1) * rows)
        two = slice((heads + head) * rows, (heads + head + 1) * rows)
        out = acc_ref[:, one] * inverse[:, one] - lambda_ref[head] * (
            acc_ref[:, two] * inverse[:, two]
        )
        mean = jnp.mean(out * out, axis=0, keepdims=True)
        attend_out.append(((out * lax.rsqrt(mean + norm_eps)).T * gain_ref[...]).astype(bf16))
    total = jnp.dot(recur_out, recur_w_ref[...], preferred_element_type=f32) + jnp.dot(
        jnp.concatenate(attend_out, axis=1), attend_w_ref[...], preferred_element_type=f32
    )
    keep_low = lax.axis_index("tp") == 0
    half = rows // 2
    keep_ref[...] = jnp.where(keep_low, total[:half], total[half:])
    send_ref[...] = jnp.where(keep_low, total[half:], total[:half]).astype(bf16)


def last_part(lambdas, gain, wide, halves, step, state, cum, local, recur_w, attend_w):
    rows, cols = cum.shape[0], recur_w.shape[1]
    return pl.pallas_call(
        functools.partial(last_kernel, step=step),
        out_shape=(
            jax.ShapeDtypeStruct((rows // 2, cols), f32),
            jax.ShapeDtypeStruct((rows // 2, cols), bf16),
        ),
        in_specs=[SMEM] + [VMEM] * 11,
        out_specs=(VMEM, VMEM),
        scratch_shapes=[pltpu.VMEM(a.shape, f32) for a in state]
        + attend_scratch(2 * halves[1].shape[0]),
        compiler_params=PARAMS,
        name="last_part",
        cost_estimate=pl.CostEstimate(flops=4 << 30, bytes_accessed=4 << 20, transcendentals=0),
    )(lambdas, gain, wide, *halves, *state, cum, local, recur_w, attend_w)


def norm_kernel(keep_ref, got_ref, gain_ref, out_ref):
    merged = keep_ref[...] + got_ref[...].astype(f32)
    mean = jnp.mean(merged * merged, axis=1, keepdims=True)
    out_ref[...] = (merged * lax.rsqrt(mean + norm_eps) * gain_ref[...]).astype(bf16)


def final_norm(keep, got, gain):
    return pl.pallas_call(
        norm_kernel,
        out_shape=jax.ShapeDtypeStruct(keep.shape, bf16),
        in_specs=[VMEM] * 3,
        out_specs=VMEM,
        compiler_params=PARAMS,
        name="final_norm",
    )(keep, got, gain)


def negative_expm1(y):
    series = 1.0 + y * (1.0 / 8.0)
    for k in (7, 6, 5, 4, 3, 2):
        series = 1.0 + y * (1.0 / k) * series
    return jnp.where(y > -0.5, -y * series, 1.0 - jnp.exp(y))


def packed(value):
    rows = []
    for _ in range(3):
        term = value.astype(bf16).astype(f32)
        value = value - term
        rows += [term[:, :256], term[:, 256:]]
    return rows


def unpacked(rows):
    rows = rows.astype(f32)
    sums = []
    for at in (0, 6):
        halves = [
            rows[at + half : at + half + 1]
            + rows[at + half + 2 : at + half + 3]
            + rows[at + half + 4 : at + half + 5]
            for half in range(2)
        ]
        sums.append(jnp.concatenate(halves, axis=1))
    return sums


def written(decay, state):
    rows = packed(decay) + packed(state)
    rows += [jnp.zeros_like(rows[0])] * (EXTRA - len(rows))
    return jnp.concatenate(rows, axis=0).astype(bf16)


def in_hbm(*arrays):
    return [pltpu.with_memory_space_constraint(a, pltpu.HBM) for a in arrays]


def started(pairs, sems):
    copies = [pltpu.make_async_copy(src, dst, sems.at[i]) for i, (src, dst) in enumerate(pairs)]
    for copy in copies:
        copy.start()
    return copies


def own_kernel(
    tokens_ref, gain_ref, *refs
):
    weights, (acc_ref, square_ref, own_ref, other_ref, held_ref, gain_held, sems) = refs[:4], refs[4:]
    width = tokens_ref.shape[1]
    tp = lax.axis_index("tp")
    mine = pl.ds(pl.multiple_of(tp * width, width), width)
    theirs = pl.ds(pl.multiple_of((1 - tp) * width, width), width)
    pairs = [(tokens_ref, held_ref), (gain_ref, gain_held)]
    parts, at = [], 0
    for w_ref in weights:
        parts.append(slice(at, at + w_ref.shape[1]))
        at += w_ref.shape[1]
    pairs += [(w_ref.at[mine, :], own_ref.at[:, part]) for w_ref, part in zip(weights, parts)]
    pairs += [(w_ref.at[theirs, :], other_ref.at[:, part]) for w_ref, part in zip(weights, parts)]
    copies = started(pairs, sems)
    copies[0].wait()
    copies[1].wait()
    tokens = held_ref[...].astype(f32)
    scaled = (tokens * gain_held[:, mine]).astype(bf16)
    square_ref[...] = jnp.broadcast_to(
        jnp.sum(tokens * tokens, axis=1, keepdims=True), square_ref.shape
    )
    for copy, part in zip(copies[2:6], parts):
        copy.wait()
        acc_ref[:, part] = jnp.dot(scaled, own_ref[:, part], preferred_element_type=f32)
    for copy in copies[6:]:
        copy.wait()


def project_own(tokens, gain, *weights):
    rows, width = tokens.shape
    cols = sum(w.shape[1] for w in weights)
    half = jax.ShapeDtypeStruct((width, cols), bf16)
    return pl.pallas_call(
        own_kernel,
        out_shape=(
            jax.ShapeDtypeStruct((rows, cols), f32),
            jax.ShapeDtypeStruct((rows, 128), f32),
            half,
            half,
        ),
        in_specs=[ANY] * 6,
        out_specs=(VMEM,) * 4,
        scratch_shapes=[
            pltpu.VMEM(tokens.shape, bf16),
            pltpu.VMEM(gain.shape, f32),
            pltpu.SemaphoreType.DMA((10,)),
        ],
        compiler_params=PARAMS,
        name="project_own",
        cost_estimate=pl.CostEstimate(flops=2 << 30, bytes_accessed=4 << 20, transcendentals=0),
    )(*in_hbm(tokens, gain, *weights))


def front_kernel(
    acc_ref,
    square_ref,
    own_w_ref,
    other_w_ref,
    other_ref,
    halo_own_ref,
    halo_other_ref,
    gain_hbm,
    taps_hbm,
    decay_hbm,
    input_hbm,
    base_hbm,
    extra_hbm,
    out_recur_hbm,
    out_attend_hbm,
    piece_ref,
    wide_ref,
    cum_ref,
    state_ref,
    out_recur_ref,
    out_attend_ref,
    padded_ref,
    gain_ref,
    taps_ref,
    decay_w_ref,
    input_w_ref,
    base_ref,
    extra_ref,
    sems,
):
    rows, width = other_ref.shape
    cols = cum_ref.shape[1]
    taps = taps_ref.shape[0]
    copies = started(
        [
            (gain_hbm, gain_ref),
            (taps_hbm, taps_ref),
            (decay_hbm, decay_w_ref),
            (input_hbm, input_w_ref),
            (base_hbm, base_ref),
            (extra_hbm, extra_ref),
            (out_recur_hbm, out_recur_ref),
            (out_attend_hbm, out_attend_ref),
        ],
        sems,
    )
    tp = lax.axis_index("tp")
    mine = pl.ds(pl.multiple_of(tp * width, width), width)
    theirs = pl.ds(pl.multiple_of((1 - tp) * width, width), width)
    copies[0].wait()

    def scaled(tokens, part):
        return (tokens * gain_ref[:, part]).astype(bf16)

    other = other_ref[...].astype(f32)
    square = square_ref[:, 0:1] + jnp.sum(other * other, axis=1, keepdims=True)
    inverse = lax.rsqrt(square / D + norm_eps)
    scaled_other = scaled(other, theirs)

    def project(at, count):
        lanes = slice(at, at + count)
        part = jnp.dot(scaled_other, other_w_ref[:, lanes], preferred_element_type=f32)
        return (acc_ref[:, lanes] + part) * inverse

    halo_own, halo_other = halo_own_ref[...].astype(f32), halo_other_ref[...].astype(f32)
    square = jnp.sum(halo_own * halo_own, axis=1, keepdims=True) + jnp.sum(
        halo_other * halo_other, axis=1, keepdims=True
    )
    halo = jnp.dot(scaled(halo_own, mine), own_w_ref[:, :cols], preferred_element_type=f32)
    both = jnp.dot(
        jnp.concatenate([scaled_other, scaled(halo_other, theirs)], axis=0),
        other_w_ref[:, :cols],
        preferred_element_type=f32,
    )
    halo = ((halo + both[rows:]) * lax.rsqrt(square / D + norm_eps)).astype(bf16)
    padded_ref[0:8, :] = halo.astype(f32)
    recur_in = ((acc_ref[:, :cols] + both[:rows]) * inverse).astype(bf16)
    padded_ref[8 : 8 + rows, :] = recur_in.astype(f32)

    at = own_w_ref.shape[1] - 2 * HEAD - DV
    piece_ref[:rows, : 2 * HEAD] = project(at, 2 * HEAD).astype(bf16)
    piece_ref[:rows, 2 * HEAD :] = project(at + 2 * HEAD, DV).astype(bf16)

    queries = project(cols, at - cols).astype(bf16) * HEAD ** (-0.5)
    heads = queries.shape[1] // (2 * HEAD)
    first = lax.broadcasted_iota(jnp.int32, (rows, 2 * HEAD), 1) < HEAD
    for head in range(heads):
        part = queries[:, head * 2 * HEAD : (head + 1) * 2 * HEAD]
        zero = jnp.zeros_like(part)
        wide_ref[head * rows : (head + 1) * rows, :] = jnp.where(first, part, zero)
        begin = (heads + head) * rows
        wide_ref[begin : begin + rows, :] = jnp.where(first, zero, part)

    for copy in copies[1:6]:
        copy.wait()
    extra_decay = extra_ref[...].T
    row = lax.broadcasted_iota(jnp.int32, (rows, 128), 0)
    low = lax.broadcasted_iota(jnp.int32, (rows, 128), 1) < HEAD
    square = lax.broadcasted_iota(jnp.int32, (128, 128), 0) < HEAD
    same = square == (lax.broadcasted_iota(jnp.int32, (128, 128), 1) < HEAD)
    totals = []
    for pair in range(cols // 128):
        lanes = slice(pair * 128, (pair + 1) * 128)
        conv = jnp.zeros((rows, 128), f32)
        for tap in range(taps):
            begin = 8 - (taps - 1) + tap
            conv = conv + taps_ref[tap : tap + 1, lanes] * padded_ref[begin : begin + rows, lanes]
        conv_in = conv.astype(bf16)

        def gate(w_ref):
            both = jnp.concatenate([w_ref[2 * pair], w_ref[2 * pair + 1]], axis=0)
            both = jnp.concatenate([both, both], axis=1)
            both = jnp.where(same, both, jnp.zeros_like(both))
            return jax.nn.sigmoid(jnp.dot(conv_in, both, preferred_element_type=f32))

        decay_gate = gate(decay_w_ref)
        input_gate = gate(input_w_ref)
        extra = jnp.where(
            low,
            extra_decay[:, 2 * pair : 2 * pair + 1],
            extra_decay[:, 2 * pair + 1 : 2 * pair + 2],
        )
        log_decay = -lru_rate * decay_gate * base_ref[:, lanes] - extra
        decay = jnp.exp(log_decay)
        inject = jnp.sqrt(negative_expm1(2.0 * log_decay)) * input_gate * conv_in.astype(f32)
        step = 1
        while step < rows:
            if step < 8:
                keep = row >= step
                decay_before = jnp.where(keep, pltpu.roll(decay, step, 0), 1.0)
                inject_before = jnp.where(keep, pltpu.roll(inject, step, 0), 0.0)
            else:
                one = jnp.ones((step, 128), f32)
                decay_before = jnp.concatenate([one, decay[:-step]], axis=0)
                inject_before = jnp.concatenate([jnp.zeros_like(one), inject[:-step]], axis=0)
            inject = inject + decay * inject_before
            decay = decay * decay_before
            step *= 2
        cum_ref[:, lanes] = decay
        state_ref[:, lanes] = inject
        totals.append((decay[rows - 1 :], inject[rows - 1 :]))
    decay, state = (jnp.concatenate(t, axis=1) for t in zip(*totals))
    piece_ref[rows:, :] = written(decay, state)
    for copy in copies[6:]:
        copy.wait()


def front(own, other, halos, small, out_weights, cols):
    rows = other.shape[0]
    queries = own[0].shape[1] - cols - 2 * HEAD - DV
    whole = jax.ShapeDtypeStruct((rows, cols), f32)
    return pl.pallas_call(
        front_kernel,
        out_shape=(
            jax.ShapeDtypeStruct((rows + EXTRA, 2 * HEAD + DV), bf16),
            jax.ShapeDtypeStruct((2 * rows * queries // (2 * HEAD), 2 * HEAD), bf16),
            whole,
            whole,
            *(jax.ShapeDtypeStruct(w.shape, bf16) for w in out_weights),
        ),
        in_specs=[VMEM] * 7 + [ANY] * 8,
        out_specs=(VMEM,) * 6,
        scratch_shapes=[pltpu.VMEM((rows + 8, cols), f32)]
        + [pltpu.VMEM(a.shape, a.dtype) for a in small]
        + [pltpu.SemaphoreType.DMA((8,))],
        compiler_params=PARAMS,
        name="front",
        cost_estimate=pl.CostEstimate(flops=4 << 30, bytes_accessed=1 << 20, transcendentals=0),
    )(*own, other, *halos, *in_hbm(*small, *out_weights))


def assemble_kernel(*refs):
    pieces, (block_ref, one_ref, two_ref, carry_ref, each_ref) = refs[:NY], refs[NY:]
    rows = pieces[0].shape[0] - EXTRA
    for r, piece in enumerate(pieces):
        begin = EXTRA + r * rows
        block_ref[begin : begin + rows, :] = piece[:rows, :]
        half_ref, begin = (one_ref, begin) if r < NY // 2 else (two_ref, (r - NY // 2) * rows)
        half_ref[begin : begin + rows, :] = piece[:rows, :]
        decay, state = unpacked(piece[rows:, :])
        each_ref[r, 0:1, :] = decay
        each_ref[r, 1:2, :] = state
    own_y = lax.axis_index("sp") % NY
    decay, state = each_ref[own_y, 0:1, :], each_ref[own_y, 1:2, :]
    before = [jnp.ones_like(decay), jnp.zeros_like(state)]
    for y in range(1, NY):
        earlier = y - 1 < own_y
        before = [
            jnp.where(earlier, decay, before[0]),
            jnp.where(earlier, state, before[1]),
        ]
        earlier = y <= own_y
        at = lax.rem(own_y - y + NY, NY)
        this = each_ref[at, 0:1, :]
        state = this * state + each_ref[at, 1:2, :]
        decay = this * decay
    block_ref[:EXTRA, :] = one_ref[:EXTRA, :] = written(decay, state)
    carry_ref[...] = jnp.zeros_like(carry_ref)
    carry_ref[0:1, :] = before[0]
    carry_ref[1:2, :] = before[1]
    carry_ref[2:3, :] = jnp.ones_like(decay)


def assemble(pieces, cols):
    rows, width = pieces[0].shape
    return pl.pallas_call(
        assemble_kernel,
        out_shape=(
            jax.ShapeDtypeStruct((NY * (rows - EXTRA) + EXTRA, width), bf16),
            jax.ShapeDtypeStruct((NY // 2 * (rows - EXTRA) + EXTRA, width), bf16),
            jax.ShapeDtypeStruct((NY // 2 * (rows - EXTRA), width), bf16),
            jax.ShapeDtypeStruct((8, cols), f32),
        ),
        in_specs=[VMEM] * NY,
        out_specs=(VMEM,) * 4,
        scratch_shapes=[pltpu.VMEM((NY, 8, cols), f32)],
        compiler_params=PARAMS,
        name="assemble",
    )(*pieces)


def layer(
    tokens,
    norm_gain,
    w_recur_in,
    conv_weight,
    w_gate_decay,
    w_gate_input,
    decay_base,
    extra_decay,
    w_query,
    w_key,
    w_value,
    mix_lambda,
    head_gain,
    w_out_recur,
    w_out_attend,
    out_gain,
):
    rows = tokens.shape[0]
    recur_cols = w_recur_in.shape[1]
    weights = (w_recur_in, w_query, w_key, w_value)
    gain = norm_gain[None, :]

    swap = [(0, 1), (1, 0)]
    other = lax.ppermute(tokens, "tp", swap)
    ends = tokens[rows - 8 :]
    halo_own = lax.ppermute(ends, ("sp", "tp"), later(0))
    halo_other = lax.ppermute(ends, ("sp", "tp"), later(1))
    own = project_own(tokens, gain, *weights)
    small = (gain, conv_weight, w_gate_decay, w_gate_input, decay_base[None, :], extra_decay.T)
    piece, wide, cum, local, w_out_recur, w_out_attend = front(
        own, other, (halo_own, halo_other), small, (w_out_recur, w_out_attend), recur_cols
    )

    pieces = [piece] + [lax.ppermute(piece, "sp", sp_pairs(0, r)) for r in range(1, NY)]
    block, *same, carry = assemble(pieces, recur_cols)

    state = (*attend_first(wide, block), carry)
    cross = lax.ppermute(block, "tp", swap)
    waiting = []
    for step in range(1, NZ // 2 + 1):
        for i in range(2):
            same[i] = lax.ppermute(same[i], ("sp", "tp"), around())
        if step == NZ // 2:
            break
        waiting.append((tuple(same), step, 0))
        state = attend_more(wide, waiting, state)
        cross = lax.ppermute(cross, ("sp", "tp"), around())
        other = lax.ppermute(cross, "tp", swap)
        waiting = [((other,), step, 1)]
    state = attend_more(wide, waiting, state)
    keep, send = last_part(
        mix_lambda,
        head_gain[None, :],
        wide,
        same,
        NZ // 2,
        state,
        cum,
        local,
        w_out_recur,
        w_out_attend,
    )
    got = lax.ppermute(send, "tp", swap)
    return final_norm(keep, got, out_gain[None, :])


def solution(mesh):
    in_specs = (
        P(("fs", "sp"), "tp"),
        P(),
        P(None, "tp"),
        P(None, "tp"),
        P("tp", None, None),
        P("tp", None, None),
        P("tp"),
        P(("fs", "sp"), "tp"),
        P(None, "tp"),
        P(None, "tp"),
        P(None, "tp"),
        P("tp"),
        P(),
        P("tp", None),
        P("tp", None),
        P(),
    )
    out_specs = P(("fs", "sp", "tp"), None)
    return jax.shard_map(layer, mesh=mesh, in_specs=in_specs, out_specs=out_specs, check_vma=False)
```

```python
import functools

import jax
import jax.numpy as jnp
from jax import lax
from jax.experimental import pallas as pl
from jax.experimental.pallas import tpu as pltpu
from jax.sharding import PartitionSpec as P


D = 2048
HEAD = 64
DV = 128
NY = 4
NZ = 8
lru_rate = 8.0
norm_eps = 1e-06
COLS = 128
EXTRA = 16
f32 = jnp.float32
bf16 = jnp.bfloat16


def sp_pairs(dz, dy):
    return [
        (z * NY + y, (z + dz) % NZ * NY + (y + dy) % NY) for z in range(NZ) for y in range(NY)
    ]


def around():
    return [
        (2 * i + t, 2 * ((z + 1 - 2 * t) % NZ * NY + y) + t)
        for i in range(NZ * NY)
        for z, y in [divmod(i, NY)]
        for t in range(2)
    ]


def along_y(piece, distance):
    return lax.ppermute(piece, "sp", sp_pairs(0, distance))


def later(flip):
    return [(2 * i + t, 2 * i + 2 + (t ^ flip)) for i in range(NZ * NY - 1) for t in range(2)]


def attend_block(kv, q_ref, acc_ref, stat_ref, score_ref, expo_ref, mask=None):
    keys = kv[:, : 2 * HEAD]
    values_t = kv[:, 2 * HEAD :].T
    cols = score_ref.shape[2]
    steps = q_ref.shape[0] // cols

    def score(i):
        score_ref[i % 2] = lax.dot_general(
            keys,
            q_ref[i * cols : (i + 1) * cols, :],
            (((1,), (1,)), ((), ())),
            preferred_element_type=f32,
        )

    def soften(i):
        part = slice(i * cols, (i + 1) * cols)
        scores = score_ref[i % 2]
        if mask is not None:
            scores = jnp.where(mask, scores, -1e30)
        old = stat_ref[0:1, part]
        peak = jnp.maximum(old, jnp.max(scores, axis=0, keepdims=True))
        fix = jnp.exp(old - peak)
        expo = jnp.exp(scores - peak)
        stat_ref[0:1, part] = peak
        stat_ref[1:2, part] = stat_ref[1:2, part] * fix + jnp.sum(expo, axis=0, keepdims=True)
        expo_ref[i % 2] = expo.astype(bf16)
        acc_ref[:, part] = acc_ref[:, part] * fix

    def gain(i):
        part = slice(i * cols, (i + 1) * cols)
        acc_ref[:, part] += jnp.dot(values_t, expo_ref[i % 2], preferred_element_type=f32)

    score(0)
    for i in range(steps):
        if i + 1 < steps:
            score(i + 1)
        soften(i)
        if i > 0:
            gain(i - 1)
    gain(steps - 1)


def attend_scratch(keys):
    return [pltpu.VMEM((2, keys, COLS), f32), pltpu.VMEM((2, keys, COLS), bf16)]


def first_kernel(
    wide_ref,
    block_ref,
    acc_ref,
    stat_ref,
    score_ref,
    expo_ref,
):
    rows = wide_ref.shape[0] // 8
    acc_ref[...] = jnp.zeros_like(acc_ref)
    stat_ref[...] = jnp.zeros_like(stat_ref)
    stat_ref[0:1, :] = jnp.full((1, stat_ref.shape[1]), -1e30, f32)
    count, cols = NY * rows, COLS
    key_at = lax.broadcasted_iota(jnp.int32, (count, cols), 0)
    query_at = lax.broadcasted_iota(jnp.int32, (count, cols), 1) % rows
    own_y = lax.axis_index("sp") % NY
    mask = key_at <= jnp.where(key_at < rows, query_at, own_y * rows + rows - 1)
    attend_block(block_ref[EXTRA:, :], wide_ref, acc_ref, stat_ref, score_ref, expo_ref, mask)


def take_block(step, up, parts, wide_ref, acc_ref, stat_ref, carry_ref, score_ref, expo_ref):
    own_z = lax.axis_index("sp") // NY
    needed = jnp.where(up, own_z, own_z + 2 * step - NZ) >= step

    @pl.when(needed)
    def _():
        block = jnp.concatenate([parts[0][EXTRA:, :]] + [part[...] for part in parts[1:]], axis=0)
        attend_block(block, wide_ref, acc_ref, stat_ref, score_ref, expo_ref)

    @pl.when(jnp.logical_and(needed, up))
    def _():
        decay, state = unpacked(parts[0][:EXTRA, :])
        before = carry_ref[0:1, :]
        carry_ref[1:2, :] = before * state + carry_ref[1:2, :]
        carry_ref[0:1, :] = before * decay

    @pl.when(jnp.logical_and(needed, jnp.logical_not(up)))
    def _():
        decay, state = unpacked(parts[0][:EXTRA, :])
        carry_ref[3:4, :] = decay * carry_ref[3:4, :] + state
        carry_ref[2:3, :] = decay * carry_ref[2:3, :]


def more_kernel(wide_ref, *refs, steps):
    n = sum(count for _, _, count in steps)
    blocks, (acc_in, stat_in, carry_in) = list(refs[:n]), refs[n : n + 3]
    acc_ref, stat_ref, carry_ref, score_ref, expo_ref = refs[n + 3 :]
    acc_ref[...] = acc_in[...]
    stat_ref[...] = stat_in[...]
    carry_ref[...] = carry_in[...]
    core = lax.axis_index("tp")
    refs = (wide_ref, acc_ref, stat_ref, carry_ref, score_ref, expo_ref)
    for step, up_core, count in steps:
        parts, blocks = blocks[:count], blocks[count:]
        take_block(step, core == up_core, parts, *refs)


PARAMS = pltpu.CompilerParams(vmem_limit_bytes=16 << 20)
VMEM = pl.BlockSpec(memory_space=pltpu.VMEM)
ANY = pl.BlockSpec(memory_space=pltpu.HBM)


def attend_first(wide, block):
    return pl.pallas_call(
        first_kernel,
        out_shape=(
            jax.ShapeDtypeStruct((DV, wide.shape[0]), f32),
            jax.ShapeDtypeStruct((8, wide.shape[0]), f32),
        ),
        in_specs=[VMEM] * 2,
        out_specs=(VMEM,) * 2,
        scratch_shapes=attend_scratch(block.shape[0] - EXTRA),
        compiler_params=PARAMS,
        name="attend_first",
        cost_estimate=pl.CostEstimate(flops=4 << 30, bytes_accessed=1 << 20, transcendentals=0),
    )(wide, block)


def attend_more(wide, waiting, state):
    blocks = [part for parts, _, _ in waiting for part in parts]
    steps = tuple((step, up_core, len(parts)) for parts, step, up_core in waiting)
    n = len(blocks)
    return pl.pallas_call(
        functools.partial(more_kernel, steps=steps),
        out_shape=tuple(jax.ShapeDtypeStruct(a.shape, f32) for a in state),
        in_specs=[VMEM] * (n + 4),
        out_specs=(VMEM,) * 3,
        input_output_aliases={n + 1: 0, n + 2: 1, n + 3: 2},
        scratch_shapes=attend_scratch(sum(part.shape[0] for part in waiting[0][0]) - EXTRA),
        compiler_params=PARAMS,
        name="attend_more",
        cost_estimate=pl.CostEstimate(flops=4 << 30, bytes_accessed=1 << 20, transcendentals=0),
    )(wide, *blocks, *state)


def last_kernel(
    lambda_ref,
    gain_ref,
    wide_ref,
    one_ref,
    two_ref,
    acc_in,
    stat_in,
    carry_in,
    cum_ref,
    local_ref,
    recur_w_ref,
    attend_w_ref,
    keep_ref,
    send_ref,
    acc_ref,
    stat_ref,
    carry_ref,
    score_ref,
    expo_ref,
    *,
    step,
):
    acc_ref[...] = acc_in[...]
    stat_ref[...] = stat_in[...]
    carry_ref[...] = carry_in[...]
    refs = (wide_ref, acc_ref, stat_ref, carry_ref, score_ref, expo_ref)
    take_block(step, lax.axis_index("tp") >= 0, (one_ref, two_ref), *refs)
    before = carry_ref[0:1, :] * carry_ref[3:4, :] + carry_ref[1:2, :]
    recur_out = (local_ref[...] + cum_ref[...] * before).astype(bf16)
    rows = recur_out.shape[0]
    heads = acc_ref.shape[1] // (2 * rows)
    inverse = 1.0 / stat_ref[1:2, :]
    attend_out = []
    for head in range(heads):
        one = slice(head * rows, (head + 1) * rows)
        two = slice((heads + head) * rows, (heads + head + 1) * rows)
        out = acc_ref[:, one] * inverse[:, one] - lambda_ref[0:1, head : head + 1] * (
            acc_ref[:, two] * inverse[:, two]
        )
        mean = jnp.mean(out * out, axis=0, keepdims=True)
        attend_out.append(((out * lax.rsqrt(mean + norm_eps)).T * gain_ref[...]).astype(bf16))
    total = jnp.dot(recur_out, recur_w_ref[...], preferred_element_type=f32) + jnp.dot(
        jnp.concatenate(attend_out, axis=1), attend_w_ref[...], preferred_element_type=f32
    )
    keep_low = lax.axis_index("tp") == 0
    half = rows // 2
    keep_ref[...] = jnp.where(keep_low, total[:half], total[half:])
    send_ref[...] = jnp.where(keep_low, total[half:], total[:half]).astype(bf16)


def last_part(lambdas, gain, wide, halves, step, state, cum, local, recur_w, attend_w):
    rows, cols = cum.shape[0], recur_w.shape[1]
    return pl.pallas_call(
        functools.partial(last_kernel, step=step),
        out_shape=(
            jax.ShapeDtypeStruct((rows // 2, cols), f32),
            jax.ShapeDtypeStruct((rows // 2, cols), bf16),
        ),
        in_specs=[VMEM] * 12,
        out_specs=(VMEM, VMEM),
        scratch_shapes=[pltpu.VMEM(a.shape, f32) for a in state]
        + attend_scratch(2 * halves[1].shape[0]),
        compiler_params=PARAMS,
        name="last_part",
        cost_estimate=pl.CostEstimate(flops=4 << 30, bytes_accessed=4 << 20, transcendentals=0),
    )(lambdas, gain, wide, *halves, *state, cum, local, recur_w, attend_w)


def norm_kernel(keep_ref, got_ref, gain_ref, out_ref):
    merged = keep_ref[...] + got_ref[...].astype(f32)
    mean = jnp.mean(merged * merged, axis=1, keepdims=True)
    out_ref[...] = (merged * lax.rsqrt(mean + norm_eps) * gain_ref[...]).astype(bf16)


def final_norm(keep, got, gain):
    return pl.pallas_call(
        norm_kernel,
        out_shape=jax.ShapeDtypeStruct(keep.shape, bf16),
        in_specs=[VMEM] * 3,
        out_specs=VMEM,
        compiler_params=PARAMS,
        name="final_norm",
    )(keep, got, gain)


def negative_expm1(y):
    series = 1.0 + y * (1.0 / 8.0)
    for k in (7, 6, 5, 4, 3, 2):
        series = 1.0 + y * (1.0 / k) * series
    return jnp.where(y > -0.5, -y * series, 1.0 - jnp.exp(y))


def packed(value):
    rows = []
    for _ in range(3):
        term = value.astype(bf16).astype(f32)
        value = value - term
        rows += [term[:, :256], term[:, 256:]]
    return rows


def unpacked(rows):
    rows = rows.astype(f32)
    sums = []
    for at in (0, 6):
        halves = [
            rows[at + half : at + half + 1]
            + rows[at + half + 2 : at + half + 3]
            + rows[at + half + 4 : at + half + 5]
            for half in range(2)
        ]
        sums.append(jnp.concatenate(halves, axis=1))
    return sums


def written(decay, state):
    rows = packed(decay) + packed(state)
    rows += [jnp.zeros_like(rows[0])] * (EXTRA - len(rows))
    return jnp.concatenate(rows, axis=0).astype(bf16)


def in_hbm(*arrays):
    return [pltpu.with_memory_space_constraint(a, pltpu.HBM) for a in arrays]


def started(pairs, sems):
    copies = [pltpu.make_async_copy(src, dst, sems.at[i]) for i, (src, dst) in enumerate(pairs)]
    for copy in copies:
        copy.start()
    return copies


def own_kernel(
    tokens_ref, gain_ref, *refs
):
    weights, (acc_ref, square_ref, own_ref, other_ref, held_ref, gain_held, sems) = refs[:4], refs[4:]
    width = tokens_ref.shape[1]
    tp = lax.axis_index("tp")
    mine = pl.ds(pl.multiple_of(tp * width, width), width)
    theirs = pl.ds(pl.multiple_of((1 - tp) * width, width), width)
    pairs = [(tokens_ref, held_ref), (gain_ref, gain_held)]
    parts, at = [], 0
    for w_ref in weights:
        parts.append(slice(at, at + w_ref.shape[1]))
        at += w_ref.shape[1]
    pairs += [(w_ref.at[mine, :], own_ref.at[:, part]) for w_ref, part in zip(weights, parts)]
    pairs += [(w_ref.at[theirs, :], other_ref.at[:, part]) for w_ref, part in zip(weights, parts)]
    copies = started(pairs, sems)
    copies[0].wait()
    copies[1].wait()
    tokens = held_ref[...].astype(f32)
    scaled = (tokens * gain_held[:, mine]).astype(bf16)
    square_ref[...] = jnp.broadcast_to(
        jnp.sum(tokens * tokens, axis=1, keepdims=True), square_ref.shape
    )
    for copy, part in zip(copies[2:6], parts):
        copy.wait()
        acc_ref[:, part] = jnp.dot(scaled, own_ref[:, part], preferred_element_type=f32)
    for copy in copies[6:]:
        copy.wait()


def project_own(tokens, gain, *weights):
    rows, width = tokens.shape
    cols = sum(w.shape[1] for w in weights)
    half = jax.ShapeDtypeStruct((width, cols), bf16)
    return pl.pallas_call(
        own_kernel,
        out_shape=(
            jax.ShapeDtypeStruct((rows, cols), f32),
            jax.ShapeDtypeStruct((rows, 128), f32),
            half,
            half,
        ),
        in_specs=[ANY] * 6,
        out_specs=(VMEM,) * 4,
        scratch_shapes=[
            pltpu.VMEM(tokens.shape, bf16),
            pltpu.VMEM(gain.shape, f32),
            pltpu.SemaphoreType.DMA((10,)),
        ],
        compiler_params=PARAMS,
        name="project_own",
        cost_estimate=pl.CostEstimate(flops=2 << 30, bytes_accessed=4 << 20, transcendentals=0),
    )(*in_hbm(tokens, gain, *weights))


def front_kernel(
    acc_ref,
    square_ref,
    own_w_ref,
    other_w_ref,
    other_ref,
    halo_own_ref,
    halo_other_ref,
    gain_hbm,
    taps_hbm,
    decay_hbm,
    input_hbm,
    base_hbm,
    extra_hbm,
    out_recur_hbm,
    out_attend_hbm,
    lambda_hbm,
    head_gain_hbm,
    out_gain_hbm,
    piece_ref,
    scaled_ref,
    inverse_ref,
    cum_ref,
    state_ref,
    out_recur_ref,
    out_attend_ref,
    lambda_ref,
    head_gain_ref,
    out_gain_ref,
    padded_ref,
    gain_ref,
    taps_ref,
    decay_w_ref,
    input_w_ref,
    base_ref,
    extra_ref,
    sems,
):
    rows, width = other_ref.shape
    cols = cum_ref.shape[1]
    taps = taps_ref.shape[0]
    copies = started(
        [
            (gain_hbm, gain_ref),
            (taps_hbm, taps_ref),
            (decay_hbm, decay_w_ref),
            (input_hbm, input_w_ref),
            (base_hbm, base_ref),
            (extra_hbm, extra_ref),
            (out_recur_hbm, out_recur_ref),
            (out_attend_hbm, out_attend_ref),
            (lambda_hbm, lambda_ref),
            (head_gain_hbm, head_gain_ref),
            (out_gain_hbm, out_gain_ref),
        ],
        sems,
    )
    tp = lax.axis_index("tp")
    mine = pl.ds(pl.multiple_of(tp * width, width), width)
    theirs = pl.ds(pl.multiple_of((1 - tp) * width, width), width)
    copies[0].wait()

    def scaled(tokens, part):
        return (tokens * gain_ref[:, part]).astype(bf16)

    other = other_ref[...].astype(f32)
    square = square_ref[:, 0:1] + jnp.sum(other * other, axis=1, keepdims=True)
    inverse = lax.rsqrt(square / D + norm_eps)
    scaled_other = scaled(other, theirs)
    scaled_ref[...] = scaled_other
    inverse_ref[...] = jnp.broadcast_to(inverse, inverse_ref.shape)

    def project(at, count):
        lanes = slice(at, at + count)
        part = jnp.dot(scaled_other, other_w_ref[:, lanes], preferred_element_type=f32)
        return (acc_ref[:, lanes] + part) * inverse

    halo_own, halo_other = halo_own_ref[...].astype(f32), halo_other_ref[...].astype(f32)
    square = jnp.sum(halo_own * halo_own, axis=1, keepdims=True) + jnp.sum(
        halo_other * halo_other, axis=1, keepdims=True
    )
    halo = jnp.dot(scaled(halo_own, mine), own_w_ref[:, :cols], preferred_element_type=f32)
    both = jnp.dot(
        jnp.concatenate([scaled_other, scaled(halo_other, theirs)], axis=0),
        other_w_ref[:, :cols],
        preferred_element_type=f32,
    )
    halo = ((halo + both[rows:]) * lax.rsqrt(square / D + norm_eps)).astype(bf16)
    padded_ref[0:8, :] = halo.astype(f32)
    recur_in = ((acc_ref[:, :cols] + both[:rows]) * inverse).astype(bf16)
    padded_ref[8 : 8 + rows, :] = recur_in.astype(f32)

    at = own_w_ref.shape[1] - 2 * HEAD - DV
    piece_ref[:rows, : 2 * HEAD] = project(at, 2 * HEAD).astype(bf16)
    piece_ref[:rows, 2 * HEAD :] = project(at + 2 * HEAD, DV).astype(bf16)

    for copy in copies[1:6]:
        copy.wait()
    extra_decay = extra_ref[...].T
    row = lax.broadcasted_iota(jnp.int32, (rows, 128), 0)
    low = lax.broadcasted_iota(jnp.int32, (rows, 128), 1) < HEAD
    square = lax.broadcasted_iota(jnp.int32, (128, 128), 0) < HEAD
    same = square == (lax.broadcasted_iota(jnp.int32, (128, 128), 1) < HEAD)
    totals = []
    for pair in range(cols // 128):
        lanes = slice(pair * 128, (pair + 1) * 128)
        conv = jnp.zeros((rows, 128), f32)
        for tap in range(taps):
            begin = 8 - (taps - 1) + tap
            conv = conv + taps_ref[tap : tap + 1, lanes] * padded_ref[begin : begin + rows, lanes]
        conv_in = conv.astype(bf16)

        def gate(w_ref):
            both = jnp.concatenate([w_ref[2 * pair], w_ref[2 * pair + 1]], axis=0)
            both = jnp.concatenate([both, both], axis=1)
            both = jnp.where(same, both, jnp.zeros_like(both))
            return jax.nn.sigmoid(jnp.dot(conv_in, both, preferred_element_type=f32))

        decay_gate = gate(decay_w_ref)
        input_gate = gate(input_w_ref)
        extra = jnp.where(
            low,
            extra_decay[:, 2 * pair : 2 * pair + 1],
            extra_decay[:, 2 * pair + 1 : 2 * pair + 2],
        )
        log_decay = -lru_rate * decay_gate * base_ref[:, lanes] - extra
        decay = jnp.exp(log_decay)
        inject = jnp.sqrt(negative_expm1(2.0 * log_decay)) * input_gate * conv_in.astype(f32)
        step = 1
        while step < rows:
            if step < 8:
                keep = row >= step
                decay_before = jnp.where(keep, pltpu.roll(decay, step, 0), 1.0)
                inject_before = jnp.where(keep, pltpu.roll(inject, step, 0), 0.0)
            else:
                one = jnp.ones((step, 128), f32)
                decay_before = jnp.concatenate([one, decay[:-step]], axis=0)
                inject_before = jnp.concatenate([jnp.zeros_like(one), inject[:-step]], axis=0)
            inject = inject + decay * inject_before
            decay = decay * decay_before
            step *= 2
        cum_ref[:, lanes] = decay
        state_ref[:, lanes] = inject
        totals.append((decay[rows - 1 :], inject[rows - 1 :]))
    decay, state = (jnp.concatenate(t, axis=1) for t in zip(*totals))
    piece_ref[rows:, :] = written(decay, state)
    for copy in copies[6:]:
        copy.wait()


def front(own, other, halos, small, later_uses, cols):
    rows = other.shape[0]
    whole = jax.ShapeDtypeStruct((rows, cols), f32)
    return pl.pallas_call(
        front_kernel,
        out_shape=(
            jax.ShapeDtypeStruct((rows + EXTRA, 2 * HEAD + DV), bf16),
            jax.ShapeDtypeStruct(other.shape, bf16),
            jax.ShapeDtypeStruct((rows, 128), f32),
            whole,
            whole,
            *(jax.ShapeDtypeStruct(w.shape, w.dtype) for w in later_uses),
        ),
        in_specs=[VMEM] * 7 + [ANY] * 11,
        out_specs=(VMEM,) * 10,
        scratch_shapes=[pltpu.VMEM((rows + 8, cols), f32)]
        + [pltpu.VMEM(a.shape, a.dtype) for a in small]
        + [pltpu.SemaphoreType.DMA((11,))],
        compiler_params=PARAMS,
        name="front",
        cost_estimate=pl.CostEstimate(flops=4 << 30, bytes_accessed=1 << 20, transcendentals=0),
    )(*own, other, *halos, *in_hbm(*small, *later_uses))


def query_kernel(acc_ref, scaled_ref, inverse_ref, w_ref, wide_ref, *, begin, count):
    rows = scaled_ref.shape[0]
    lanes = slice(begin, begin + count)
    part = jnp.dot(scaled_ref[...], w_ref[:, lanes], preferred_element_type=f32)
    queries = ((acc_ref[:, lanes] + part) * inverse_ref[:, 0:1]).astype(bf16) * HEAD ** (-0.5)
    heads = count // (2 * HEAD)
    first = lax.broadcasted_iota(jnp.int32, (rows, 2 * HEAD), 1) < HEAD
    for head in range(heads):
        part = queries[:, head * 2 * HEAD : (head + 1) * 2 * HEAD]
        zero = jnp.zeros_like(part)
        wide_ref[head * rows : (head + 1) * rows, :] = jnp.where(first, part, zero)
        at = (heads + head) * rows
        wide_ref[at : at + rows, :] = jnp.where(first, zero, part)


def project_queries(acc, scaled, inverse, other_w, begin, count):
    rows = scaled.shape[0]
    return pl.pallas_call(
        functools.partial(query_kernel, begin=begin, count=count),
        out_shape=jax.ShapeDtypeStruct((count // HEAD * rows, 2 * HEAD), bf16),
        in_specs=[VMEM] * 4,
        out_specs=VMEM,
        compiler_params=PARAMS,
        name="project_queries",
        cost_estimate=pl.CostEstimate(flops=1 << 30, bytes_accessed=1 << 20, transcendentals=0),
    )(acc, scaled, inverse, other_w)


def assemble_kernel(*refs):
    pieces, (block_ref, one_ref, two_ref, carry_ref, each_ref) = refs[:NY], refs[NY:]
    rows = pieces[0].shape[0] - EXTRA
    for r, piece in enumerate(pieces):
        begin = EXTRA + r * rows
        block_ref[begin : begin + rows, :] = piece[:rows, :]
        half_ref, begin = (one_ref, begin) if r < NY // 2 else (two_ref, (r - NY // 2) * rows)
        half_ref[begin : begin + rows, :] = piece[:rows, :]
        decay, state = unpacked(piece[rows:, :])
        each_ref[r, 0:1, :] = decay
        each_ref[r, 1:2, :] = state
    own_y = lax.axis_index("sp") % NY
    decay, state = each_ref[own_y, 0:1, :], each_ref[own_y, 1:2, :]
    before = [jnp.ones_like(decay), jnp.zeros_like(state)]
    for y in range(1, NY):
        earlier = y - 1 < own_y
        before = [
            jnp.where(earlier, decay, before[0]),
            jnp.where(earlier, state, before[1]),
        ]
        earlier = y <= own_y
        at = lax.rem(own_y - y + NY, NY)
        this = each_ref[at, 0:1, :]
        state = this * state + each_ref[at, 1:2, :]
        decay = this * decay
    block_ref[:EXTRA, :] = one_ref[:EXTRA, :] = written(decay, state)
    carry_ref[...] = jnp.zeros_like(carry_ref)
    carry_ref[0:1, :] = before[0]
    carry_ref[1:2, :] = before[1]
    carry_ref[2:3, :] = jnp.ones_like(decay)


def assemble(pieces, cols):
    rows, width = pieces[0].shape
    return pl.pallas_call(
        assemble_kernel,
        out_shape=(
            jax.ShapeDtypeStruct((NY * (rows - EXTRA) + EXTRA, width), bf16),
            jax.ShapeDtypeStruct((NY // 2 * (rows - EXTRA) + EXTRA, width), bf16),
            jax.ShapeDtypeStruct((NY // 2 * (rows - EXTRA), width), bf16),
            jax.ShapeDtypeStruct((8, cols), f32),
        ),
        in_specs=[VMEM] * NY,
        out_specs=(VMEM,) * 4,
        scratch_shapes=[pltpu.VMEM((NY, 8, cols), f32)],
        compiler_params=PARAMS,
        name="assemble",
    )(*pieces)


def layer(
    tokens,
    norm_gain,
    w_recur_in,
    conv_weight,
    w_gate_decay,
    w_gate_input,
    decay_base,
    extra_decay,
    w_query,
    w_key,
    w_value,
    mix_lambda,
    head_gain,
    w_out_recur,
    w_out_attend,
    out_gain,
):
    rows = tokens.shape[0]
    recur_cols = w_recur_in.shape[1]
    weights = (w_recur_in, w_query, w_key, w_value)
    gain = norm_gain[None, :]

    swap = [(0, 1), (1, 0)]
    other = lax.ppermute(tokens, "tp", swap)
    ends = tokens[rows - 8 :]
    halo_own = lax.ppermute(ends, ("sp", "tp"), later(0))
    halo_other = lax.ppermute(ends, ("sp", "tp"), later(1))
    own = project_own(tokens, gain, *weights)
    small = (gain, conv_weight, w_gate_decay, w_gate_input, decay_base[None, :], extra_decay.T)
    later_uses = (
        w_out_recur,
        w_out_attend,
        mix_lambda[None, :],
        head_gain[None, :],
        out_gain[None, :],
    )
    piece, scaled, inverse, cum, local, *later_uses = front(
        own, other, (halo_own, halo_other), small, later_uses, recur_cols
    )
    w_out_recur, w_out_attend, lambdas, head_gain, out_gain = later_uses
    wide = project_queries(own[0], scaled, inverse, own[3], recur_cols, w_query.shape[1])

    pieces = [piece] + [along_y(piece, r) for r in range(1, NY)]
    block, *same, carry = assemble(pieces, recur_cols)

    state = (*attend_first(wide, block), carry)
    cross = lax.ppermute(block, "tp", swap)
    waiting = []
    for step in range(1, NZ // 2 + 1):
        for i in range(2):
            same[i] = lax.ppermute(same[i], ("sp", "tp"), around())
        if step == NZ // 2:
            break
        waiting.append((tuple(same), step, 0))
        state = attend_more(wide, waiting, state)
        cross = lax.ppermute(cross, ("sp", "tp"), around())
        other = lax.ppermute(cross, "tp", swap)
        waiting = [((other,), step, 1)]
    state = attend_more(wide, waiting, state)
    keep, send = last_part(
        lambdas,
        head_gain,
        wide,
        same,
        NZ // 2,
        state,
        cum,
        local,
        w_out_recur,
        w_out_attend,
    )
    got = lax.ppermute(send, "tp", swap)
    return final_norm(keep, got, out_gain)


def solution(mesh):
    in_specs = (
        P(("fs", "sp"), "tp"),
        P(),
        P(None, "tp"),
        P(None, "tp"),
        P("tp", None, None),
        P("tp", None, None),
        P("tp"),
        P(("fs", "sp"), "tp"),
        P(None, "tp"),
        P(None, "tp"),
        P(None, "tp"),
        P("tp"),
        P(),
        P("tp", None),
        P("tp", None),
        P(),
    )
    out_specs = P(("fs", "sp", "tp"), None)
    return jax.shard_map(layer, mesh=mesh, in_specs=in_specs, out_specs=out_specs, check_vma=False)
```
